512 devices in a mesh: fs: 128 (over z, x, core), tp: 4 (over y).
Axes of the slice: x: 4, y: 4, z: 16, core: 2. Of those that a mesh axis runs over, the one named last changes fastest.
Arguments:
- normed_input: bfloat16 [81920, 2048], P('fs'), may hold values from -448 to 448
- key_cotangent: bfloat16 [81920, 512], P('fs', 'tp'), may hold values from -0.01953125 to 0.01953125
- value_cotangent: bfloat16 [81920, 1024], P('fs', 'tp'), may hold values from -0.01953125 to 0.01953125
- key_factor: bfloat16 [512, 128], P('tp'), may hold values from -2.8 to 2.8
- value_factor: bfloat16 [1024, 128], P('tp'), may hold values from -2.8 to 2.8
- key_weight: float32 [2048, 512], P('fs', 'tp'), may hold values from -0.125 to 0.125
- value_weight: float32 [2048, 1024], P('fs', 'tp'), may hold values from -0.125 to 0.125
- first_moments: float32 [2, 2048, 128], P(None, 'fs', 'tp'), may hold values from -0.6 to 0.6
- second_moments: float32 [2, 2048, 128], P(None, 'fs', 'tp'), may hold values from 0.001 to 0.1
Outputs:
- first_new: float32 [2, 2048, 128], P(None, 'fs', 'tp')
- second_new: float32 [2, 2048, 128], P(None, 'fs', 'tp')
- new_key_weight: float32 [2048, 512], P('fs', 'tp')
- new_value_weight: float32 [2048, 1024], P('fs', 'tp')
- key_copy: bfloat16 [2048, 512], P(None, 'tp')
- value_copy: bfloat16 [2048, 1024], P(None, 'tp')
The draws below stay inside these ranges and needn't reach their ends.
All inputs are finite; a program needn't handle non-finite values.
Results may differ from the reference program's by a relative error of at most 0.005.
Values may be sent and summed in bfloat16 or wider, within the bound.
A program may use at most 64 MiB of HBM per device.

```python
import math
import jax
import jax.numpy as jnp
from jax import lax

D = 2048
RANK = 128
TOK_DEV = 640
TOKENS = 81920
NK = 512
NV = 1024
N_FS = 128


def factor_draw(base_key, rows_total, salt_value):
    key_list = jax.random.split(jax.random.fold_in(base_key, salt_value), 2)
    column = jnp.arange(RANK).astype(jnp.float32) / RANK
    rough_scale = jax.random.uniform(key_list[0], (RANK,), jnp.float32, 0.7, 1.4)
    base_draw = jnp.clip(jax.random.normal(key_list[1], (rows_total, RANK), jnp.float32), -5.0, 5.0)
    column_ramp = 10.0 ** column
    return (0.04 * base_draw * (column_ramp * rough_scale)[None, :]).astype(jnp.bfloat16)


def draw_key_factor(key, part):
    return factor_draw(key, NK, 21)


def draw_value_factor(key, part):
    return factor_draw(key, NV, 22)


def draw_normed_input(key, part):
    key_list = jax.random.split(jax.random.fold_in(key, 11), 4)
    blocks = TOKENS // TOK_DEV
    column = jnp.arange(D).astype(jnp.float32) / D
    rough_scale = jax.random.uniform(key_list[0], (D,), jnp.float32, 0.7, 1.4)
    noise_draw = jnp.clip(jax.random.normal(key_list[1], (TOKENS, D), jnp.float32), -5.0, 5.0)
    column_ramp = 10.0 ** column
    partner = jax.random.permutation(key_list[3], blocks)
    token_block = jnp.arange(TOKENS) // TOK_DEV
    column_block = jnp.arange(D) // (D // blocks)
    boost_mask = jnp.where(partner[token_block][:, None] == column_block[None, :], 4.0, 1.0)
    return (noise_draw * (column_ramp * rough_scale)[None, :] * boost_mask).astype(jnp.bfloat16)


def shard_levels(own_key, shape, cuts, low, largest):
    def one(dim, parts):
        heights = jax.random.uniform(jax.random.fold_in(jax.random.fold_in(own_key, 6), dim), (parts,), jnp.float32, low / len(cuts), largest / len(cuts))
        return jnp.repeat(jnp.exp(heights), shape[dim] // parts).reshape((-1,) + (1,) * (len(shape) - dim - 1))

    gain = one(*cuts[0])
    for cut in cuts[1:]:
        gain = gain * one(*cut)
    return gain


def centred(own_key, dims, deviation, reach, cuts=(), held_as=jnp.bfloat16):
    array = deviation * jax.random.normal(own_key, dims, jnp.float32)
    if cuts:
        array = array * shard_levels(own_key, dims, cuts, -0.22, 0.18)
    return jnp.clip(array, -reach, reach).astype(held_as)


def setup_inputs(seed: int = 0) -> dict:
    streams_of = jax.random.split(jax.random.key(seed), 10)
    normed_input = draw_normed_input(jax.random.fold_in(streams_of[9], 71), 0)
    key_cotangent = centred(streams_of[1], (TOKENS, NK), (TOK_DEV * N_FS) ** -0.5, 0.01953125, ((0, 128), (1, 4)))
    value_cotangent = centred(streams_of[2], (TOKENS, NV), (TOK_DEV * N_FS) ** -0.5, 0.01953125, ((0, 128), (1, 4)))
    key_factor = draw_key_factor(jax.random.fold_in(streams_of[9], 71), 0)
    value_factor = draw_value_factor(jax.random.fold_in(streams_of[9], 71), 0)
    key_weight = centred(streams_of[5], (D, NK), D ** -0.5, 0.125, ((0, 128), (1, 4)), jnp.float32)
    value_weight = centred(streams_of[6], (D, NV), D ** -0.5, 0.125, ((0, 128), (1, 4)), jnp.float32)
    first_moments = centred(streams_of[7], (2, D, RANK), 0.1, 0.6, ((1, 128), (2, 4)), jnp.float32)
    second_moments = jnp.clip(jnp.exp(math.log(0.1) - 4.6051702 * jax.random.uniform(streams_of[8], (2, D, RANK), jnp.float32) ** shard_levels(streams_of[8], (2, D, RANK), ((1, 128), (2, 4)), -0.2, 0.2)), 0.001, 0.1)
    return {"normed_input": normed_input, "key_cotangent": key_cotangent, "value_cotangent": value_cotangent, "key_factor": key_factor, "value_factor": value_factor, "key_weight": key_weight, "value_weight": value_weight, "first_moments": first_moments, "second_moments": second_moments}


step_rate = 0.05
clip_target = 0.1
beta_first = 0.8
beta_second = 0.95
small_eps = 1e-08
norm_eps = 1e-06

def reference(normed_input, key_cotangent, value_cotangent, key_factor, value_factor, key_weight, value_weight, first_moments, second_moments):
    contract = (((0,), (0,)), ((), ()))
    grad_key = lax.dot_general(normed_input, key_cotangent, contract, preferred_element_type=jnp.float32)
    grad_value = lax.dot_general(normed_input, value_cotangent, contract, preferred_element_type=jnp.float32)
    proj_key = jnp.dot(grad_key, key_factor.astype(jnp.float32), precision=lax.Precision.HIGHEST)
    proj_value = jnp.dot(grad_value, value_factor.astype(jnp.float32), precision=lax.Precision.HIGHEST)
    total_sq = jnp.sum(proj_key * proj_key) + jnp.sum(proj_value * proj_value)
    clip_limit = clip_target * jnp.sqrt(jnp.float32(2 * D * RANK))
    clip_factor = jnp.minimum(1.0, clip_limit / jnp.sqrt(total_sq + norm_eps))
    scaled = clip_factor * jnp.stack([proj_key, proj_value])
    first_new = beta_first * first_moments + (1.0 - beta_first) * scaled
    second_new = beta_second * second_moments + (1.0 - beta_second) * scaled * scaled
    direction = first_new / (jnp.sqrt(second_new) + small_eps)
    back = (((1,), (1,)), ((), ()))
    update_key = lax.dot_general(direction[0], key_factor.astype(jnp.float32), back, precision=lax.Precision.HIGHEST)
    update_value = lax.dot_general(direction[1], value_factor.astype(jnp.float32), back, precision=lax.Precision.HIGHEST)
    new_key = key_weight - step_rate * update_key
    new_value = value_weight - step_rate * update_value
    return (first_new, second_new, new_key, new_value, new_key.astype(jnp.bfloat16), new_value.astype(jnp.bfloat16))
```

```python
import jax
import jax.numpy as jnp
from jax import lax
from jax.experimental import pallas as pl
from jax.experimental.pallas import tpu as pltpu
from jax.sharding import Mesh
from jax.sharding import PartitionSpec as P

D = 2048
RANK = 128
NZ, NX, NC, NY = 16, 4, 2, 4
FS = ("z", "x", "c")
TOK = 640
HALF = TOK // 2
NK = 128
NV = 256
NW = NK + NV

step_rate = 0.05
clip_target = 0.1
beta_first = 0.8
beta_second = 0.95
small_eps = 1e-08
norm_eps = 1e-06

NEAR = (1, 15, 14)
FAR = (4, 12, 8)
f32 = jnp.float32
bf16 = jnp.bfloat16


def kernel(
    x_hbm, ck_hbm, cv_hbm, fk_ref, fv_ref, kw_ref, vw_ref, m_ref, v_ref,
    first_ref, second_ref, nk_ref, nv_ref, ko_ref, vo_ref,
    x_vm, xt, ck, cv, wt, msend, yrecv, asend, crecv, xsend, xrecv, tsend, arecv, brecv, gy, mb, wb, sb,
    dirs, firsts, seconds, upd,
    in_sem, y_s, y_r, c_s, c_r, x_s, x_r, a_s, a_r, b_s, b_r, g_s, g_r, h_s, h_r,
    mf_s, mf_r, mn_s, mn_r, my_s, my_r, wf_s, wf_r, wn_s, wn_r, s_s, s_r,
    or_s, or_r, ol_s, ol_r, oc_s, oc_r,
):
    z, x, c, y = (lax.axis_index(n) for n in ("z", "x", "c", "y"))
    k, q = lax.div(z, 4), lax.rem(z, 4)
    other = 1 - c
    xc = x * 2 + c

    def zp(d):
        return lax.rem(z + d, NZ)

    def xp(d):
        return lax.rem(x + d, NX)

    def yp(d):
        return lax.rem(y + d, NY)

    def at_z(d):
        return (zp(d), x, c, y)

    def at_x(d):
        return (z, xp(d), c, y)

    def at_y(d):
        return (z, x, c, yp(d))

    partner = (z, x, other, y)

    def remote(src, dst, send, recv, to):
        return pltpu.make_async_remote_copy(
            src_ref=src, dst_ref=dst, send_sem=send, recv_sem=recv,
            device_id=to, device_id_type=pl.DeviceIdType.MESH,
        )

    loads = [
        pltpu.make_async_copy(ck_hbm, ck, in_sem.at[0]),
        pltpu.make_async_copy(cv_hbm, cv, in_sem.at[1]),
        pltpu.make_async_copy(x_hbm, x_vm, in_sem.at[2]),
    ]
    for load in loads:
        load.start()
    near_plane = [
        (z, xp(dx), c if dc == 0 else other, yp(dy))
        for dx in range(NX) for dc in range(NC) for dy in range(NY) if (dx, dc, dy) != (0, 0, 0)
    ]
    barrier = pltpu.get_barrier_semaphore()
    line = [at_z(d) for d in (8, 4, 12, 2, 14, 1, 15)]
    for peer in line + near_plane:
        pl.semaphore_signal(barrier, inc=1, device_id=peer, device_id_type=pl.DeviceIdType.MESH)

    for n, ref in enumerate((m_ref, v_ref)):
        mb[y, k, q, n] = jnp.concatenate(
            [ref[0, 0:8, :], ref[1, 0:8, :], ref[0, 8:16, :], ref[1, 8:16, :]], axis=1
        )
    wb[k, q] = jnp.concatenate([kw_ref[...], vw_ref[...]], axis=1).astype(bf16)

    fk = fk_ref[...].astype(f32)
    fv = fv_ref[...].astype(f32)
    rolled_k = [fk if s == 0 else pltpu.roll(fk, 32 * s, 1) for s in range(4)]
    rolled_v = [fv if s == 0 else pltpu.roll(fv, 32 * s, 1) for s in range(4)]
    lane_k = lax.broadcasted_iota(jnp.int32, (NK, 128), 1) // 32
    lane_v = lax.broadcasted_iota(jnp.int32, (NV, 128), 1) // 32
    for t in range(NY):
        cols = pl.ds(t * 128, 128)
        for half in range(2):
            at = 2 * half
            wt[pl.ds(half * NW, NK), cols] = jnp.where(lane_k == at, rolled_k[(at - t) % 4], 0.0).astype(bf16)
            wt[pl.ds(half * NW + NK, NV), cols] = jnp.where(
                lane_v == at + 1, rolled_v[(at + 1 - t) % 4], 0.0
            ).astype(bf16)

    loads[0].wait()
    loads[1].wait()
    lhs = jnp.concatenate([ck[0:HALF], cv[0:HALF], ck[HALF:TOK], cv[HALF:TOK]], axis=1)
    reduced = jnp.dot(lhs, wt[...], preferred_element_type=f32)
    for t in range(NY):
        msend[t] = reduced[:, t * 128 : (t + 1) * 128].astype(bf16)

    pl.semaphore_wait(barrier, len(line) + len(near_plane))

    sends = []
    tp = [remote(msend.at[yp(d)], yrecv.at[d - 1], y_s.at[d - 1], y_r.at[d - 1], at_y(d)) for d in (1, 2, 3)]
    for n in (1, 0, 2):
        tp[n].start()
    sends += tp
    m_far = [remote(mb.at[y, k, q], mb.at[y, k, q], mf_s.at[n], mf_r.at[n], at_z(d)) for n, d in enumerate(FAR)]
    w_far = [remote(wb.at[k, q], wb.at[k, q], wf_s.at[n], wf_r.at[n], at_z(d)) for n, d in enumerate(FAR)]
    for n in (2, 0, 1):
        m_far[n].start()
        w_far[n].start()
    sends += m_far + w_far

    loads[2].wait()
    for n in range(8):
        xt[pl.ds(n * 256, 256), :] = x_vm[:, n * 256 : (n + 1) * 256].T

    for copy in tp:
        copy.wait_recv()
    own = msend[y].astype(f32)
    for n in range(3):
        own = own + yrecv[n].astype(f32)
    swapped = pltpu.roll(own, 64, 1)
    low = lax.broadcasted_iota(jnp.int32, (HALF, 128), 1) < 64
    both = jnp.concatenate([jnp.where(low, own, swapped), jnp.where(low, swapped, own)], axis=0)
    upper = both.astype(bf16)
    lower = (both - upper.astype(f32)).astype(bf16)
    rhs = jnp.concatenate([upper, lower], axis=1)
    low_tile = lax.broadcasted_iota(jnp.int32, (16, 8, 128), 2) < 64
    for n in range(8):
        wide = jnp.dot(xt[pl.ds(n * 256, 256), :], rhs, preferred_element_type=f32)
        part = (wide[:, :128] + wide[:, 128:]).reshape(16, 2, 8, 128)
        packed = jnp.where(low_tile, part[:, 0], part[:, 1]).reshape(2, 8, 8, 128)
        for t in range(8):
            asend[t // 2, t % 2, pl.ds(n * 16, 16), :] = packed[:, t].reshape(16, 128).astype(bf16)

    to_core = remote(asend.at[:, other], crecv, c_s, c_r, partner)
    to_core.start()
    sends.append(to_core)
    to_core.wait_recv()
    for t in range(NX):
        xsend[t] = (asend[t, c].astype(f32) + crecv[t].astype(f32)).astype(bf16)
    to_x = [remote(xsend.at[xp(d)], xrecv.at[d - 1], x_s.at[d - 1], x_r.at[d - 1], at_x(d)) for d in (1, 2, 3)]
    for n in (1, 0, 2):
        to_x[n].start()
    sends += to_x

    for copy in m_far + w_far:
        copy.wait_recv()
    m_near = [remote(mb.at[y, :, q], mb.at[y, :, q], mn_s.at[n], mn_r.at[n], at_z(d)) for n, d in enumerate(NEAR)]
    w_near = [remote(wb.at[:, q], wb.at[:, q], wn_s.at[n], wn_r.at[n], at_z(d)) for n, d in enumerate(NEAR)]
    for n in (2, 0, 1):
        m_near[n].start()
    for n in (2, 0, 1):
        w_near[n].start()
    sends += m_near + w_near

    for copy in to_x:
        copy.wait_recv()
    total = xsend[x].astype(f32)
    for n in range(3):
        total = total + xrecv[n].astype(f32)
    tsend[...] = total.reshape(4, 32, 128).astype(bf16)

    near = [
        remote(tsend.at[lax.rem(zp(d), 4)], arecv.at[n], a_s.at[n], a_r.at[n], at_z(d)) for n, d in enumerate(NEAR)
    ]
    for n in (2, 0, 1):
        near[n].start()
    sends += near
    for copy in near:
        copy.wait_recv()
    quarter = tsend[q].astype(f32)
    for n in range(3):
        quarter = quarter + arecv[n].astype(f32)
    brecv[k] = quarter.astype(bf16)
    far = [remote(brecv.at[k], brecv.at[k], b_s.at[n], b_r.at[n], at_z(d)) for n, d in enumerate(FAR)]
    for n in (2, 0, 1):
        far[n].start()
    sends += far

    for copy in m_near:
        copy.wait_recv()
    m_tp = [remote(mb.at[y], mb.at[y], my_s.at[d - 1], my_r.at[d - 1], at_y(d)) for d in (1, 2, 3)]
    for n in (1, 0, 2):
        m_tp[n].start()
    sends += m_tp

    for copy in far:
        copy.wait_recv()
    quarter = brecv[0].astype(f32)
    for n in range(1, 4):
        quarter = quarter + brecv[n].astype(f32)
    gy[y, q] = quarter.astype(bf16)
    spread = [remote(gy.at[y, q], gy.at[y, q], g_s.at[n], g_r.at[n], at_z(d)) for n, d in enumerate(NEAR)]
    for n in (2, 0, 1):
        spread[n].start()
    sends += spread

    def to_tp(n, part):
        return [
            remote(gy.at[y, part], gy.at[y, part], h_s.at[n, d - 1], h_r.at[n, d - 1], at_y(d)) for d in (1, 2, 3)
        ]

    quarters = [q, lax.rem(zp(15), 4), lax.rem(zp(1), 4), lax.rem(zp(2), 4)]
    across = to_tp(0, quarters[0])
    for n in (1, 0, 2):
        across[n].start()
    for n in range(3):
        spread[n].wait_recv()
        more = to_tp(n + 1, quarters[n + 1])
        for i in (1, 0, 2):
            more[i].start()
        across += more
    sends += across

    mine = gy[y].astype(f32)
    me = (x * NC + c) * NY + y
    sb[me] = jnp.sum((mine * mine).reshape(128, 128), axis=0, keepdims=True)
    squares = [remote(sb.at[me], sb.at[me], s_s.at[n], s_r.at[n], to) for n, to in enumerate(near_plane)]
    for copy in squares:
        copy.start()
    sends += squares

    for copy in m_tp + w_near + squares + across:
        copy.wait_recv()

    sums = jnp.sum(sb[...], axis=0)
    total_sq = jnp.sum(sums, axis=1, keepdims=True)
    clip_limit = clip_target * jnp.sqrt(jnp.float32(2 * D * RANK))
    clip_factor = jnp.minimum(1.0, clip_limit / jnp.sqrt(total_sq + norm_eps))
    for t in range(NY):
        scaled = clip_factor * gy[t].astype(f32).reshape(128, 128)
        first_new = beta_first * mb[t, :, :, 0].reshape(128, 128) + (1.0 - beta_first) * scaled
        second_new = beta_second * mb[t, :, :, 1].reshape(128, 128) + (1.0 - beta_second) * scaled * scaled
        firsts[t] = first_new.reshape(16, 8, 128)
        seconds[t] = second_new.reshape(16, 8, 128)
        dirs[:, t * 128 : (t + 1) * 128] = first_new / (jnp.sqrt(second_new) + small_eps)

    left, right = at_x(3), at_x(1)
    xc_left, xc_right = xp(3) * 2 + c, xp(1) * 2 + c
    xc_across = xp(2) * 2 + c

    def block(ref, half, which):
        return ref.at[pl.ds(half * 8, 8), which]

    def pair(half, which, send, recv, n, to):
        return [
            remote(block(ref, half, which), block(ref, half, which), send.at[n, i], recv.at[n, i], to)
            for i, ref in enumerate((ko_ref, vo_ref))
        ]

    go_right, go_left, go_core = {}, {}, {}
    for half in range(2):
        direction = dirs[pl.ds(half * 64, 64), :]
        upper = direction.astype(bf16)
        lower = (direction - upper.astype(f32)).astype(bf16)
        product = lax.dot_general(
            jnp.concatenate([upper, lower], axis=0), wt[...], (((1,), (1,)), ((), ())), preferred_element_type=f32
        )
        product = product[0:64] + product[64:128]
        upd[pl.ds(half * 8, 8)] = product.reshape(8, 8, 2 * NW)
        old = wb[pl.ds(half * 2, 2)].reshape(8, 16, NW).astype(f32)
        moved = jnp.stack(
            [product[:, 0:NW].reshape(8, 8, NW), product[:, NW : 2 * NW].reshape(8, 8, NW)], axis=1
        ).reshape(8, 16, NW)
        new = (old - step_rate * moved).astype(bf16)
        ko_ref[pl.ds(half * 8, 8), xc] = new[:, :, 0:NK]
        vo_ref[pl.ds(half * 8, 8), xc] = new[:, :, NK:NW]
        if half == 0:
            go_right[0] = pair(0, xc, or_s, or_r, 0, right)
            go_core[0] = pair(0, xc, oc_s, oc_r, 0, partner)
            started = go_right[0] + go_core[0]
        else:
            go_left[0] = pair(1, xc, ol_s, ol_r, 0, left)
            go_left[1] = pair(0, xc, ol_s, ol_r, 1, left)
            go_right[1] = pair(1, xc, or_s, or_r, 1, right)
            go_core[1] = pair(1, xc, oc_s, oc_r, 1, partner)
            started = go_left[0] + go_right[1] + go_left[1] + go_core[1]
        for copy in started:
            copy.start()
        sends += started

    for out, packed_all in ((first_ref, firsts), (second_ref, seconds)):
        packed = packed_all[y, z]
        out[0, 0:8, :] = packed[:, 0:32]
        out[1, 0:8, :] = packed[:, 32:64]
        out[0, 8:16, :] = packed[:, 64:96]
        out[1, 8:16, :] = packed[:, 96:128]
    own_upd = upd[z]
    for half in range(2):
        rows = slice(half * 8, half * 8 + 8)
        at = half * NW
        nk_ref[rows, :] = kw_ref[rows, :] - step_rate * own_upd[:, at : at + NK]
        nv_ref[rows, :] = vw_ref[rows, :] - step_rate * own_upd[:, at + NK : at + NW]

    def arrived(pairs):
        for copy in pairs:
            copy.wait_recv()

    def forward(pairs):
        nonlocal sends
        for copy in pairs:
            copy.start()
        sends += pairs

    arrived(go_right[0])
    go_right[2] = pair(0, xc_left, or_s, or_r, 2, right)
    forward(go_right[2])
    go_core[2] = pair(0, xc_left, oc_s, oc_r, 2, partner)
    forward(go_core[2])
    arrived(go_left[0])
    go_left[2] = pair(1, xc_right, ol_s, ol_r, 2, left)
    forward(go_left[2])
    go_core[3] = pair(1, xc_right, oc_s, oc_r, 3, partner)
    forward(go_core[3])
    arrived(go_right[1])
    go_core[4] = pair(1, xc_left, oc_s, oc_r, 4, partner)
    forward(go_core[4])
    arrived(go_left[1])
    go_core[5] = pair(0, xc_right, oc_s, oc_r, 5, partner)
    forward(go_core[5])
    arrived(go_right[2])
    go_core[6] = pair(0, xc_across, oc_s, oc_r, 6, partner)
    forward(go_core[6])
    arrived(go_left[2])
    go_core[7] = pair(1, xc_across, oc_s, oc_r, 7, partner)
    forward(go_core[7])
    for n in range(8):
        arrived(go_core[n])
    for copy in sends:
        copy.wait_send()


def local(*args):
    vmem = pl.BlockSpec(memory_space=pltpu.VMEM)
    anywhere = pl.BlockSpec(memory_space=pl.ANY)
    dma = pltpu.SemaphoreType.DMA
    shape = jax.ShapeDtypeStruct
    outs = pl.pallas_call(
        kernel,
        out_shape=(
            shape((2, 16, 32), f32),
            shape((2, 16, 32), f32),
            shape((16, NK), f32),
            shape((16, NV), f32),
            shape((NZ, NX * NC, 16, NK), bf16),
            shape((NZ, NX * NC, 16, NV), bf16),
        ),
        in_specs=[anywhere] * 3 + [vmem] * 6,
        out_specs=[vmem] * 6,
        scratch_shapes=[
            pltpu.VMEM((TOK, D), bf16),
            pltpu.VMEM((D, TOK), bf16),
            pltpu.VMEM((TOK, NK), bf16),
            pltpu.VMEM((TOK, NV), bf16),
            pltpu.VMEM((2 * NW, 4 * 128), bf16),
            pltpu.VMEM((NY, HALF, 128), bf16),
            pltpu.VMEM((NY - 1, HALF, 128), bf16),
            pltpu.VMEM((NX, NC, 128, 128), bf16),
            pltpu.VMEM((NX, 128, 128), bf16),
            pltpu.VMEM((NX, 128, 128), bf16),
            pltpu.VMEM((NX - 1, 128, 128), bf16),
            pltpu.VMEM((4, 32, 128), bf16),
            pltpu.VMEM((3, 32, 128), bf16),
            pltpu.VMEM((4, 32, 128), bf16),
            pltpu.VMEM((NY, 4, 32, 128), bf16),
            pltpu.VMEM((NY, 4, 4, 2, 8, 128), f32),
            pltpu.VMEM((4, 4, 16, NW), bf16),
            pltpu.VMEM((NX * NC * NY, 1, 128), f32),
            pltpu.VMEM((128, 4 * 128), f32),
            pltpu.VMEM((NY, 16, 8, 128), f32),
            pltpu.VMEM((NY, 16, 8, 128), f32),
            pltpu.VMEM((16, 8, 2 * NW), f32),
            dma((3,)),
            dma((3,)), dma((3,)), dma, dma, dma((3,)), dma((3,)), dma((3,)), dma((3,)), dma((3,)), dma((3,)),
            dma((3,)), dma((3,)), dma((4, 3)), dma((4, 3)),
            dma((3,)), dma((3,)), dma((3,)), dma((3,)), dma((3,)), dma((3,)),
            dma((3,)), dma((3,)), dma((3,)), dma((3,)), dma((31,)), dma((31,)),
            dma((3, 2)), dma((3, 2)), dma((3, 2)), dma((3, 2)), dma((8, 2)), dma((8, 2)),
        ],
        compiler_params=pltpu.CompilerParams(
            collective_id=0, has_side_effects=True, vmem_limit_bytes=40 * 1024 * 1024
        ),
        name="step",
    )(*args)
    first_new, second_new, new_key, new_value, key_copy, value_copy = outs
    return first_new, second_new, new_key, new_value, key_copy.reshape(D, NK), value_copy.reshape(D, NV)


def solution(mesh):
    torus = Mesh(mesh.devices.reshape(NZ, NX, NC, NY), ("z", "x", "c", "y"))
    return jax.shard_map(
        local,
        mesh=torus,
        in_specs=(
            P(FS, None), P(FS, "y"), P(FS, "y"), P("y", None), P("y", None), P(FS, "y"), P(FS, "y"),
            P(None, FS, "y"), P(None, FS, "y"),
        ),
        out_specs=(P(None, FS, "y"), P(None, FS, "y"), P(FS, "y"), P(FS, "y"), P(None, "y"), P(None, "y")),
        check_vma=False,
    )
```

```python
import jax
import jax.numpy as jnp
from jax import lax
from jax.experimental import pallas as pl
from jax.experimental.pallas import tpu as pltpu
from jax.sharding import Mesh
from jax.sharding import PartitionSpec as P

D = 2048
RANK = 128
NZ, NX, NC, NY = 16, 4, 2, 4
FS = ("z", "x", "c")
TOK = 640
HALF = TOK // 2
NK = 128
NV = 256
NW = NK + NV

step_rate = 0.05
clip_target = 0.1
beta_first = 0.8
beta_second = 0.95
small_eps = 1e-08
norm_eps = 1e-06

NEAR = (1, 15, 14)
FAR = (4, 12, 8)
f32 = jnp.float32
bf16 = jnp.bfloat16


def kernel(
    x_hbm, ck_hbm, cv_hbm, fk_hbm, fv_hbm, kw_hbm, vw_hbm, m_hbm, v_hbm,
    first_ref, second_ref, nk_ref, nv_ref, ko_ref, vo_ref,
    x_vm, xt, ck, cv, wt, msend, yrecv, asend, crecv, xsend, xrecv, tsend, arecv, brecv, gy, mb, wb, sb,
    dirs, firsts, seconds, upd, fk_ref, fv_ref, kw_ref, vw_ref, m_ref, v_ref,
    in_sem, y_s, y_r, c_s, c_r, x_s, x_r, a_s, a_r, b_s, b_r, g_s, g_r, h_s, h_r,
    mf_s, mf_r, mn_s, mn_r, my_s, my_r, wf_s, wf_r, wn_s, wn_r, s_s, s_r,
    or_s, or_r, ol_s, ol_r, oc_s, oc_r,
):
    z, x, c, y = (lax.axis_index(n) for n in ("z", "x", "c", "y"))
    k, q = lax.div(z, 4), lax.rem(z, 4)
    other = 1 - c
    xc = x * 2 + c

    def zp(d):
        return lax.rem(z + d, NZ)

    def xp(d):
        return lax.rem(x + d, NX)

    def yp(d):
        return lax.rem(y + d, NY)

    def at_z(d):
        return (zp(d), x, c, y)

    def at_x(d):
        return (z, xp(d), c, y)

    def at_y(d):
        return (z, x, c, yp(d))

    partner = (z, x, other, y)

    def remote(src, dst, send, recv, to):
        return pltpu.make_async_remote_copy(
            src_ref=src, dst_ref=dst, send_sem=send, recv_sem=recv,
            device_id=to, device_id_type=pl.DeviceIdType.MESH,
        )

    loads = [
        pltpu.make_async_copy(src, dst, in_sem.at[n])
        for n, (src, dst) in enumerate([
            (fk_hbm, fk_ref), (fv_hbm, fv_ref), (ck_hbm, ck), (cv_hbm, cv),
            (m_hbm, m_ref), (v_hbm, v_ref), (kw_hbm, kw_ref), (vw_hbm, vw_ref), (x_hbm, x_vm),
        ])
    ]
    for load in loads:
        load.start()
    near_plane = [
        (z, xp(dx), c if dc == 0 else other, yp(dy))
        for dx in range(NX) for dc in range(NC) for dy in range(NY) if (dx, dc, dy) != (0, 0, 0)
    ]
    barrier = pltpu.get_barrier_semaphore()
    line = [at_z(d) for d in (8, 4, 12, 2, 14, 1, 15)]
    for peer in line + near_plane:
        pl.semaphore_signal(barrier, inc=1, device_id=peer, device_id_type=pl.DeviceIdType.MESH)

    with jax.named_scope("w_factor"):
        loads[0].wait()
        loads[1].wait()
    fk = fk_ref[...].astype(f32)
    fv = fv_ref[...].astype(f32)
    rolled_k = [fk if s == 0 else pltpu.roll(fk, 32 * s, 1) for s in range(4)]
    rolled_v = [fv if s == 0 else pltpu.roll(fv, 32 * s, 1) for s in range(4)]
    lane_k = lax.broadcasted_iota(jnp.int32, (NK, 128), 1) // 32
    lane_v = lax.broadcasted_iota(jnp.int32, (NV, 128), 1) // 32
    for t in range(NY):
        cols = pl.ds(t * 128, 128)
        for half in range(2):
            at = 2 * half
            wt[pl.ds(half * NW, NK), cols] = jnp.where(lane_k == at, rolled_k[(at - t) % 4], 0.0).astype(bf16)
            wt[pl.ds(half * NW + NK, NV), cols] = jnp.where(
                lane_v == at + 1, rolled_v[(at + 1 - t) % 4], 0.0
            ).astype(bf16)

    with jax.named_scope("w_cot"):
        loads[2].wait()
        loads[3].wait()
    lhs = jnp.concatenate([ck[0:HALF], cv[0:HALF], ck[HALF:TOK], cv[HALF:TOK]], axis=1)
    reduced = jnp.dot(lhs, wt[...], preferred_element_type=f32)
    for t in range(NY):
        msend[t] = reduced[:, t * 128 : (t + 1) * 128].astype(bf16)

    for load in loads[4:8]:
        load.wait()
    for n, ref in enumerate((m_ref, v_ref)):
        mb[y, k, q, n] = jnp.concatenate(
            [ref[0, 0:8, :], ref[1, 0:8, :], ref[0, 8:16, :], ref[1, 8:16, :]], axis=1
        )
    wb[k, q] = jnp.concatenate([kw_ref[...], vw_ref[...]], axis=1).astype(bf16)

    with jax.named_scope("w_barrier"):
        pl.semaphore_wait(barrier, len(line) + len(near_plane))

    sends = []
    tp = [remote(msend.at[yp(d)], yrecv.at[d - 1], y_s.at[d - 1], y_r.at[d - 1], at_y(d)) for d in (1, 2, 3)]
    for n in (1, 0, 2):
        tp[n].start()
    sends += tp
    m_far = [remote(mb.at[y, k, q], mb.at[y, k, q], mf_s.at[n], mf_r.at[n], at_z(d)) for n, d in enumerate(FAR)]
    w_far = [remote(wb.at[k, q], wb.at[k, q], wf_s.at[n], wf_r.at[n], at_z(d)) for n, d in enumerate(FAR)]
    for n in (2, 0, 1):
        m_far[n].start()
        w_far[n].start()
    sends += m_far + w_far

    loads[8].wait()
    for n in range(8):
        xt[pl.ds(n * 256, 256), :] = x_vm[:, n * 256 : (n + 1) * 256].T

    with jax.named_scope("w_tp"):
        for copy in tp:
            copy.wait_recv()
    own = msend[y].astype(f32)
    for n in range(3):
        own = own + yrecv[n].astype(f32)
    swapped = pltpu.roll(own, 64, 1)
    low = lax.broadcasted_iota(jnp.int32, (HALF, 128), 1) < 64
    both = jnp.concatenate([jnp.where(low, own, swapped), jnp.where(low, swapped, own)], axis=0)
    upper = both.astype(bf16)
    lower = (both - upper.astype(f32)).astype(bf16)
    rhs = jnp.concatenate([upper, lower], axis=1)
    low_tile = lax.broadcasted_iota(jnp.int32, (16, 8, 128), 2) < 64
    for n in range(8):
        wide = jnp.dot(xt[pl.ds(n * 256, 256), :], rhs, preferred_element_type=f32)
        part = (wide[:, :128] + wide[:, 128:]).reshape(16, 2, 8, 128)
        packed = jnp.where(low_tile, part[:, 0], part[:, 1]).reshape(2, 8, 8, 128)
        for t in range(8):
            asend[t // 2, t % 2, pl.ds(n * 16, 16), :] = packed[:, t].reshape(16, 128).astype(bf16)

    to_core = remote(asend.at[:, other], crecv, c_s, c_r, partner)
    to_core.start()
    sends.append(to_core)
    with jax.named_scope("w_core"):
        to_core.wait_recv()
    for t in range(NX):
        xsend[t] = (asend[t, c].astype(f32) + crecv[t].astype(f32)).astype(bf16)
    to_x = [remote(xsend.at[xp(d)], xrecv.at[d - 1], x_s.at[d - 1], x_r.at[d - 1], at_x(d)) for d in (1, 2, 3)]
    for n in (1, 0, 2):
        to_x[n].start()
    sends += to_x

    with jax.named_scope("w_bg_far"):
        for copy in m_far + w_far:
            copy.wait_recv()
    m_near = [remote(mb.at[y, :, q], mb.at[y, :, q], mn_s.at[n], mn_r.at[n], at_z(d)) for n, d in enumerate(NEAR)]
    w_near = [remote(wb.at[:, q], wb.at[:, q], wn_s.at[n], wn_r.at[n], at_z(d)) for n, d in enumerate(NEAR)]
    for n in (2, 0, 1):
        m_near[n].start()
    for n in (2, 0, 1):
        w_near[n].start()
    sends += m_near + w_near

    with jax.named_scope("w_x"):
        for copy in to_x:
            copy.wait_recv()
    total = xsend[x].astype(f32)
    for n in range(3):
        total = total + xrecv[n].astype(f32)
    tsend[...] = total.reshape(4, 32, 128).astype(bf16)

    near = [
        remote(tsend.at[lax.rem(zp(d), 4)], arecv.at[n], a_s.at[n], a_r.at[n], at_z(d)) for n, d in enumerate(NEAR)
    ]
    for n in (2, 0, 1):
        near[n].start()
    sends += near
    with jax.named_scope("w_a"):
        for copy in near:
            copy.wait_recv()
    quarter = tsend[q].astype(f32)
    for n in range(3):
        quarter = quarter + arecv[n].astype(f32)
    brecv[k] = quarter.astype(bf16)
    far = [remote(brecv.at[k], brecv.at[k], b_s.at[n], b_r.at[n], at_z(d)) for n, d in enumerate(FAR)]
    for n in (2, 0, 1):
        far[n].start()
    sends += far

    with jax.named_scope("w_bg_near"):
        for copy in m_near:
            copy.wait_recv()
    m_tp = [remote(mb.at[y], mb.at[y], my_s.at[d - 1], my_r.at[d - 1], at_y(d)) for d in (1, 2, 3)]
    for n in (1, 0, 2):
        m_tp[n].start()
    sends += m_tp

    with jax.named_scope("w_b"):
        for copy in far:
            copy.wait_recv()
    quarter = brecv[0].astype(f32)
    for n in range(1, 4):
        quarter = quarter + brecv[n].astype(f32)
    gy[y, q] = quarter.astype(bf16)
    spread = [remote(gy.at[y, q], gy.at[y, q], g_s.at[n], g_r.at[n], at_z(d)) for n, d in enumerate(NEAR)]
    for n in (2, 0, 1):
        spread[n].start()
    sends += spread

    def to_tp(n, part):
        return [
            remote(gy.at[y, part], gy.at[y, part], h_s.at[n, d - 1], h_r.at[n, d - 1], at_y(d)) for d in (1, 2, 3)
        ]

    quarters = [q, lax.rem(zp(15), 4), lax.rem(zp(1), 4), lax.rem(zp(2), 4)]
    across = to_tp(0, quarters[0])
    for n in (1, 0, 2):
        across[n].start()
    for n in range(3):
        with jax.named_scope(f"w_c{n}"):
            spread[n].wait_recv()
        more = to_tp(n + 1, quarters[n + 1])
        for i in (1, 0, 2):
            more[i].start()
        across += more
    sends += across

    mine = gy[y].astype(f32)
    me = (x * NC + c) * NY + y
    sb[me] = jnp.sum((mine * mine).reshape(128, 128), axis=0, keepdims=True)
    squares = [remote(sb.at[me], sb.at[me], s_s.at[n], s_r.at[n], to) for n, to in enumerate(near_plane)]
    for copy in squares:
        copy.start()
    sends += squares

    with jax.named_scope("w_bg_y"):
        for copy in m_tp + w_near:
            copy.wait_recv()
    with jax.named_scope("w_y"):
        for copy in across:
            copy.wait_recv()
    with jax.named_scope("w_s"):
        for copy in squares:
            copy.wait_recv()

    sums = jnp.sum(sb[...], axis=0)
    total_sq = jnp.sum(sums, axis=1, keepdims=True)
    clip_limit = clip_target * jnp.sqrt(jnp.float32(2 * D * RANK))
    clip_factor = jnp.minimum(1.0, clip_limit / jnp.sqrt(total_sq + norm_eps))
    for t in range(NY):
        scaled = clip_factor * gy[t].astype(f32).reshape(128, 128)
        first_new = beta_first * mb[t, :, :, 0].reshape(128, 128) + (1.0 - beta_first) * scaled
        second_new = beta_second * mb[t, :, :, 1].reshape(128, 128) + (1.0 - beta_second) * scaled * scaled
        firsts[t] = first_new.reshape(16, 8, 128)
        seconds[t] = second_new.reshape(16, 8, 128)
        dirs[:, t * 128 : (t + 1) * 128] = first_new / (jnp.sqrt(second_new) + small_eps)

    left, right = at_x(3), at_x(1)
    xc_left, xc_right = xp(3) * 2 + c, xp(1) * 2 + c
    xc_across = xp(2) * 2 + c

    def block(ref, half, which):
        return ref.at[pl.ds(half * 8, 8), which]

    def pair(half, which, send, recv, n, to):
        return [
            remote(block(ref, half, which), block(ref, half, which), send.at[n, i], recv.at[n, i], to)
            for i, ref in enumerate((ko_ref, vo_ref))
        ]

    go_right, go_left, go_core = {}, {}, {}
    for half in range(2):
        direction = dirs[pl.ds(half * 64, 64), :]
        upper = direction.astype(bf16)
        lower = (direction - upper.astype(f32)).astype(bf16)
        product = lax.dot_general(
            jnp.concatenate([upper, lower], axis=0), wt[...], (((1,), (1,)), ((), ())), preferred_element_type=f32
        )
        product = product[0:64] + product[64:128]
        upd[pl.ds(half * 8, 8)] = product.reshape(8, 8, 2 * NW)
        old = wb[pl.ds(half * 2, 2)].reshape(8, 16, NW).astype(f32)
        moved = jnp.stack(
            [product[:, 0:NW].reshape(8, 8, NW), product[:, NW : 2 * NW].reshape(8, 8, NW)], axis=1
        ).reshape(8, 16, NW)
        new = (old - step_rate * moved).astype(bf16)
        ko_ref[pl.ds(half * 8, 8), xc] = new[:, :, 0:NK]
        vo_ref[pl.ds(half * 8, 8), xc] = new[:, :, NK:NW]
        if half == 0:
            go_right[0] = pair(0, xc, or_s, or_r, 0, right)
            go_core[0] = pair(0, xc, oc_s, oc_r, 0, partner)
            started = go_right[0] + go_core[0]
        else:
            go_left[0] = pair(1, xc, ol_s, ol_r, 0, left)
            go_left[1] = pair(0, xc, ol_s, ol_r, 1, left)
            go_right[1] = pair(1, xc, or_s, or_r, 1, right)
            go_core[1] = pair(1, xc, oc_s, oc_r, 1, partner)
            started = go_left[0] + go_right[1] + go_left[1] + go_core[1]
        for copy in started:
            copy.start()
        sends += started

    for out, packed_all in ((first_ref, firsts), (second_ref, seconds)):
        packed = packed_all[y, z]
        out[0, 0:8, :] = packed[:, 0:32]
        out[1, 0:8, :] = packed[:, 32:64]
        out[0, 8:16, :] = packed[:, 64:96]
        out[1, 8:16, :] = packed[:, 96:128]
    own_upd = upd[z]
    for half in range(2):
        rows = slice(half * 8, half * 8 + 8)
        at = half * NW
        nk_ref[rows, :] = kw_ref[rows, :] - step_rate * own_upd[:, at : at + NK]
        nv_ref[rows, :] = vw_ref[rows, :] - step_rate * own_upd[:, at + NK : at + NW]

    def arrived(pairs):
        for copy in pairs:
            copy.wait_recv()

    def forward(pairs):
        nonlocal sends
        for copy in pairs:
            copy.start()
        sends += pairs

    with jax.named_scope("w_o0"):
        arrived(go_right[0])
    go_right[2] = pair(0, xc_left, or_s, or_r, 2, right)
    forward(go_right[2])
    go_core[2] = pair(0, xc_left, oc_s, oc_r, 2, partner)
    forward(go_core[2])
    with jax.named_scope("w_o1"):
        arrived(go_left[0])
    go_left[2] = pair(1, xc_right, ol_s, ol_r, 2, left)
    forward(go_left[2])
    go_core[3] = pair(1, xc_right, oc_s, oc_r, 3, partner)
    forward(go_core[3])
    with jax.named_scope("w_o2"):
        arrived(go_right[1])
    go_core[4] = pair(1, xc_left, oc_s, oc_r, 4, partner)
    forward(go_core[4])
    with jax.named_scope("w_o3"):
        arrived(go_left[1])
    go_core[5] = pair(0, xc_right, oc_s, oc_r, 5, partner)
    forward(go_core[5])
    with jax.named_scope("w_o4"):
        arrived(go_right[2])
    go_core[6] = pair(0, xc_across, oc_s, oc_r, 6, partner)
    forward(go_core[6])
    with jax.named_scope("w_o5"):
        arrived(go_left[2])
    go_core[7] = pair(1, xc_across, oc_s, oc_r, 7, partner)
    forward(go_core[7])
    with jax.named_scope("w_oc"):
        for n in range(8):
            arrived(go_core[n])
    with jax.named_scope("w_sends"):
        for copy in sends:
            copy.wait_send()


def store(*refs):
    sems = refs[-1]
    count = (len(refs) - 1) // 2
    copies = [pltpu.make_async_copy(refs[n], refs[count + n], sems.at[n]) for n in range(count)]
    for copy in reversed(copies):
        copy.start()
    for copy in copies:
        copy.wait()


def local(*args):
    vmem = pl.BlockSpec(memory_space=pltpu.VMEM)
    hbm = pl.BlockSpec(memory_space=pltpu.HBM)
    dma = pltpu.SemaphoreType.DMA
    shape = jax.ShapeDtypeStruct
    outs = pl.pallas_call(
        kernel,
        out_shape=(
            shape((2, 16, 32), f32),
            shape((2, 16, 32), f32),
            shape((16, NK), f32),
            shape((16, NV), f32),
            shape((NZ, NX * NC, 16, NK), bf16),
            shape((NZ, NX * NC, 16, NV), bf16),
        ),
        in_specs=[hbm] * 9,
        out_specs=[vmem] * 6,
        scratch_shapes=[
            pltpu.VMEM((TOK, D), bf16),
            pltpu.VMEM((D, TOK), bf16),
            pltpu.VMEM((TOK, NK), bf16),
            pltpu.VMEM((TOK, NV), bf16),
            pltpu.VMEM((2 * NW, 4 * 128), bf16),
            pltpu.VMEM((NY, HALF, 128), bf16),
            pltpu.VMEM((NY - 1, HALF, 128), bf16),
            pltpu.VMEM((NX, NC, 128, 128), bf16),
            pltpu.VMEM((NX, 128, 128), bf16),
            pltpu.VMEM((NX, 128, 128), bf16),
            pltpu.VMEM((NX - 1, 128, 128), bf16),
            pltpu.VMEM((4, 32, 128), bf16),
            pltpu.VMEM((3, 32, 128), bf16),
            pltpu.VMEM((4, 32, 128), bf16),
            pltpu.VMEM((NY, 4, 32, 128), bf16),
            pltpu.VMEM((NY, 4, 4, 2, 8, 128), f32),
            pltpu.VMEM((4, 4, 16, NW), bf16),
            pltpu.VMEM((NX * NC * NY, 1, 128), f32),
            pltpu.VMEM((128, 4 * 128), f32),
            pltpu.VMEM((NY, 16, 8, 128), f32),
            pltpu.VMEM((NY, 16, 8, 128), f32),
            pltpu.VMEM((16, 8, 2 * NW), f32),
            pltpu.VMEM((NK, RANK), bf16),
            pltpu.VMEM((NV, RANK), bf16),
            pltpu.VMEM((16, NK), f32),
            pltpu.VMEM((16, NV), f32),
            pltpu.VMEM((2, 16, 32), f32),
            pltpu.VMEM((2, 16, 32), f32),
            dma((9,)),
            dma((3,)), dma((3,)), dma, dma, dma((3,)), dma((3,)), dma((3,)), dma((3,)), dma((3,)), dma((3,)),
            dma((3,)), dma((3,)), dma((4, 3)), dma((4, 3)),
            dma((3,)), dma((3,)), dma((3,)), dma((3,)), dma((3,)), dma((3,)),
            dma((3,)), dma((3,)), dma((3,)), dma((3,)), dma((31,)), dma((31,)),
            dma((3, 2)), dma((3, 2)), dma((3, 2)), dma((3, 2)), dma((8, 2)), dma((8, 2)),
        ],
        compiler_params=pltpu.CompilerParams(
            collective_id=0, has_side_effects=True, vmem_limit_bytes=40 * 1024 * 1024
        ),
        name="step",
    )(*[pltpu.with_memory_space_constraint(a, pltpu.HBM) for a in args])
    results = (*outs[:4], outs[4].reshape(D, NK), outs[5].reshape(D, NV))
    return pl.pallas_call(
        store,
        out_shape=tuple(shape(r.shape, r.dtype) for r in results),
        in_specs=[pl.BlockSpec(memory_space=pl.ANY)] * 6,
        out_specs=[hbm] * 6,
        scratch_shapes=[dma((6,))],
        compiler_params=pltpu.CompilerParams(vmem_limit_bytes=1024 * 1024),
        name="store",
    )(*results)


def solution(mesh):
    torus = Mesh(mesh.devices.reshape(NZ, NX, NC, NY), ("z", "x", "c", "y"))
    return jax.shard_map(
        local,
        mesh=torus,
        in_specs=(
            P(FS, None), P(FS, "y"), P(FS, "y"), P("y", None), P("y", None), P(FS, "y"), P(FS, "y"),
            P(None, FS, "y"), P(None, FS, "y"),
        ),
        out_specs=(P(None, FS, "y"), P(None, FS, "y"), P(FS, "y"), P(FS, "y"), P(None, "y"), P(None, "y")),
        check_vma=False,
    )
```

```python
import jax
import jax.numpy as jnp
from jax import lax
from jax.experimental import pallas as pl
from jax.experimental.pallas import tpu as pltpu
from jax.sharding import Mesh
from jax.sharding import PartitionSpec as P

D = 2048
RANK = 128
NZ, NX, NC, NY = 16, 4, 2, 4
FS = ("z", "x", "c")
TOK = 640
HALF = TOK // 2
NK = 128
NV = 256
NW = NK + NV

step_rate = 0.05
clip_target = 0.1
beta_first = 0.8
beta_second = 0.95
small_eps = 1e-08
norm_eps = 1e-06

FAR = (4, 12, 8)
f32 = jnp.float32
bf16 = jnp.bfloat16


def kernel(
    x_hbm, ck_hbm, cv_hbm, fk_hbm, fv_hbm, kw_hbm, vw_hbm, m_hbm, v_hbm,
    first_ref, second_ref, nk_ref, nv_ref, ko_ref, vo_ref,
    x_vm, xt, ckv, fkv, kvw, mv, wt, msend, yrecv, asend, crecv, xsend, xrecv, tsend, arecv, brecv, gy, mb, wb, s1b, s2b,
    firsts, seconds, upd,
    in_sem, c_s, c_r, x_s, x_r, g_r, o_s, o_r, one_s, one_r,
):
    z, x, c, y = (lax.axis_index(n) for n in ("z", "x", "c", "y"))
    k, q = lax.div(z, 4), lax.rem(z, 4)
    other = 1 - c
    xc = x * 2 + c

    def zp(d):
        return lax.rem(z + d, NZ)

    def xp(d):
        return lax.rem(x + d, NX)

    def yp(d):
        return lax.rem(y + d, NY)

    def at_z(d):
        return (zp(d), x, c, y)

    def at_x(d):
        return (z, xp(d), c, y)

    def at_y(d):
        return (z, x, c, yp(d))

    partner = (z, x, other, y)

    def remote(src, dst, send, recv, to):
        return pltpu.make_async_remote_copy(
            src_ref=src, dst_ref=dst, send_sem=send, recv_sem=recv,
            device_id=to, device_id_type=pl.DeviceIdType.MESH,
        )

    names = ("tp", "a", "b", "g", "h", "s1", "s2", "mf", "mn", "my", "wf", "wn")
    send_sem = {name: one_s.at[n] for n, name in enumerate(names)}
    recv_sem = {name: one_r.at[n] for n, name in enumerate(names)}
    finish = []

    def stage(name, copies, whole):
        made = [remote(src, dst, send_sem[name], recv_sem[name], to) for src, dst, to in copies]
        for copy in made:
            copy.start()
        total = remote(whole, whole, send_sem[name], recv_sem[name], partner)
        finish.append(total)
        return total

    load_f = [pltpu.make_async_copy(fk_hbm, fkv.at[pl.ds(0, NK)], in_sem.at[0]),
              pltpu.make_async_copy(fv_hbm, fkv.at[pl.ds(NK, NV)], in_sem.at[0])]
    load_c = [pltpu.make_async_copy(ck_hbm, ckv.at[:, pl.ds(0, NK)], in_sem.at[1]),
              pltpu.make_async_copy(cv_hbm, ckv.at[:, pl.ds(NK, NV)], in_sem.at[1])]
    load_x = pltpu.make_async_copy(x_hbm, x_vm, in_sem.at[2])
    load_m = [pltpu.make_async_copy(m_hbm, mv.at[0], in_sem.at[3]),
              pltpu.make_async_copy(v_hbm, mv.at[1], in_sem.at[3])]
    load_w = [pltpu.make_async_copy(kw_hbm, kvw.at[:, pl.ds(0, NK)], in_sem.at[4]),
              pltpu.make_async_copy(vw_hbm, kvw.at[:, pl.ds(NK, NV)], in_sem.at[4])]

    for load in load_f + load_c:
        load.start()
    plane = [
        (z, xp(dx), c if dc == 0 else other, y)
        for dx in range(NX) for dc in range(NC) if (dx, dc) != (0, 0)
    ]
    around = [(zp(dz), x, c, yp(dy)) for dz in (14, 1, 15, 0) for dy in (2, 1, 3, 0) if (dz, dy) != (0, 0)]
    sources = plane + [at_z(d) for d in FAR]
    sources += [(zp(dz), x, c, yp(dy)) for dz in (2, 15, 1, 0) for dy in range(NY) if (dz, dy) != (0, 0)]
    barrier = pltpu.get_barrier_semaphore()
    for peer in sources:
        pl.semaphore_signal(barrier, inc=1, device_id=peer, device_id_type=pl.DeviceIdType.MESH)
    for load in load_m + load_w + [load_x]:
        load.start()

    with jax.named_scope("w_factor"):
        pltpu.make_async_copy(fkv, fkv, in_sem.at[0]).wait()
    factor = fkv[...].astype(f32)
    rolled = [factor if s == 0 else pltpu.roll(factor, 32 * s, 1) for s in range(4)]
    lane_group = lax.broadcasted_iota(jnp.int32, (NW, 128), 1) // 32
    is_value = (lax.broadcasted_iota(jnp.int32, (NW, 128), 0) >= NK).astype(jnp.int32)
    for half in range(2):
        keep = lane_group == 2 * half + is_value
        for t in range(NY):
            at = (2 * half - t) % 4
            placed = jnp.concatenate([rolled[at][0:NK], rolled[(at + 1) % 4][NK:NW]], axis=0)
            wt[pl.ds(half * NW, NW), pl.ds(t * 128, 128)] = jnp.where(keep, placed, 0.0).astype(bf16)

    with jax.named_scope("w_cot"):
        pltpu.make_async_copy(ckv, ckv, in_sem.at[1]).wait()
    lhs = jnp.concatenate([ckv[0:HALF], ckv[HALF:TOK]], axis=1)
    reduced = jnp.dot(lhs, wt[...], preferred_element_type=f32)
    for t in range(NY):
        msend[t] = reduced[:, t * 128 : (t + 1) * 128].astype(bf16)

    pltpu.make_async_copy(mv, mv, in_sem.at[3]).wait()
    pltpu.make_async_copy(kvw, kvw, in_sem.at[4]).wait()
    for n in range(2):
        mb[y, k, q, n] = jnp.concatenate(
            [mv[n, 0, 0:8, :], mv[n, 1, 0:8, :], mv[n, 0, 8:16, :], mv[n, 1, 8:16, :]], axis=1
        )
    wb[k, q] = kvw[...].astype(bf16)

    with jax.named_scope("w_barrier"):
        pl.semaphore_wait(barrier, len(sources))

    tp = stage("tp", [(msend.at[yp(d)], yrecv.at[d - 1], at_y(d)) for d in (2, 1, 3)], yrecv)
    m_far = stage("mf", [(mb.at[y, k, q], mb.at[y, k, q], at_z(d)) for d in (8, 4, 12)], mb.at[0, 0, pl.ds(0, 3)])
    w_far = stage("wf", [(wb.at[k, q], wb.at[k, q], at_z(d)) for d in (8, 4, 12)], wb.at[0, pl.ds(0, 3)])

    load_x.wait()
    for n in range(8):
        xt[pl.ds(n * 256, 256), :] = x_vm[:, n * 256 : (n + 1) * 256].T

    with jax.named_scope("w_tp"):
        tp.wait_recv()
    own = msend[y].astype(f32)
    for n in range(3):
        own = own + yrecv[n].astype(f32)
    swapped = pltpu.roll(own, 64, 1)
    low = lax.broadcasted_iota(jnp.int32, (HALF, 128), 1) < 64
    both = jnp.concatenate([jnp.where(low, own, swapped), jnp.where(low, swapped, own)], axis=0)
    upper = both.astype(bf16)
    lower = (both - upper.astype(f32)).astype(bf16)
    rhs = jnp.concatenate([upper, lower], axis=1)
    low_tile = lax.broadcasted_iota(jnp.int32, (16, 8, 128), 2) < 64

    order = (14, 1, 15, 0)
    quarters = [lax.rem(zp(d), 4) for d in order]

    def product_of(n):
        for half in range(2):
            rows = pl.ds(pl.multiple_of(quarters[n] * 512 + half * 256, 256), 256)
            wide = jnp.dot(xt[rows, :], rhs, preferred_element_type=f32)
            part = (wide[:, :128] + wide[:, 128:]).reshape(16, 2, 8, 128)
            packed = jnp.where(low_tile, part[:, 0], part[:, 1]).reshape(2, 8, 8, 128)
            for t in range(8):
                asend[n, t // 2, t % 2, pl.ds(half * 16, 16), :] = packed[:, t].reshape(16, 128).astype(bf16)
        copy = remote(asend.at[n, :, other], crecv.at[n], c_s.at[n], c_r.at[n], partner)
        copy.start()
        return copy

    to_core, to_x = [], []

    def core_to_x(n):
        with jax.named_scope(f"w_core{n}"):
            to_core[n].wait_recv()
        for t in range(NX):
            xsend[n, t] = (asend[n, t, c].astype(f32) + crecv[n, t].astype(f32)).astype(bf16)
        for d in (2, 1, 3):
            remote(xsend.at[n, xp(d)], xrecv.at[n, d - 1], x_s.at[n], x_r.at[n], at_x(d)).start()
        to_x.append(remote(xrecv.at[n], xrecv.at[n], x_s.at[n], x_r.at[n], partner))

    to_core.append(product_of(0))
    for n in range(1, 4):
        to_core.append(product_of(n))
        core_to_x(n - 1)
    core_to_x(3)

    with jax.named_scope("w_bg_far"):
        m_far.wait_recv()
    m_near = stage("mn", [(mb.at[y, :, q], mb.at[y, :, q], at_z(d)) for d in (14, 1, 15)], mb.at[0, pl.ds(0, 3)])

    near = []
    for n in range(4):
        with jax.named_scope(f"w_x{n}"):
            to_x[n].wait_recv()
        total = xsend[n, x].astype(f32)
        for i in range(3):
            total = total + xrecv[n, i].astype(f32)
        if n < 3:
            tsend[n] = total.astype(bf16)
            remote(tsend.at[n], arecv.at[n], send_sem["a"], recv_sem["a"], at_z(order[n])).start()
    near = remote(arecv, arecv, send_sem["a"], recv_sem["a"], partner)

    with jax.named_scope("w_bg_near"):
        m_near.wait_recv()
    m_tp = stage("my", [(mb.at[y], mb.at[y], at_y(d)) for d in (2, 1, 3)], mb.at[pl.ds(0, 3)])

    with jax.named_scope("w_a"):
        near.wait_recv()
    for n in range(3):
        total = total + arecv[n].astype(f32)
    brecv[k] = total.astype(bf16)
    far = stage("b", [(brecv.at[k], brecv.at[k], at_z(d)) for d in (8, 4, 12)], brecv.at[pl.ds(0, 3)])
    with jax.named_scope("w_bg_wf"):
        w_far.wait_recv()
    with jax.named_scope("w_b"):
        far.wait_recv()
    total = brecv[0].astype(f32)
    for n in range(1, 4):
        total = total + brecv[n].astype(f32)
    rounded = total.astype(bf16)
    gy[y, q] = rounded
    rounded = rounded.astype(f32)

    s1b[xc] = jnp.sum(rounded * rounded, axis=0, keepdims=True)
    squares = stage("s1", [(s1b.at[xc], s1b.at[xc], to) for to in plane], s1b.at[pl.ds(0, 7)])

    def to_tp(part):
        return [(gy.at[y, part], gy.at[y, part], at_y(d)) for d in (2, 1, 3)]

    def start_tp(part):
        for src, dst, to in to_tp(part):
            remote(src, dst, send_sem["h"], recv_sem["h"], to).start()

    spread = [remote(gy.at[y, q], gy.at[y, q], send_sem["g"], g_r.at[n], at_z(d)) for n, d in enumerate((14, 1, 15))]
    for copy in spread:
        copy.start()
    start_tp(q)
    across = remote(gy.at[pl.ds(0, 3)], gy.at[pl.ds(0, 3)], send_sem["h"], recv_sem["h"], partner)
    for n, d in ((1, 15), (2, 1)):
        with jax.named_scope(f"w_c{n}"):
            spread[n].wait_recv()
        start_tp(lax.rem(zp(d), 4))
    with jax.named_scope("w_s1"):
        squares.wait_recv()
    row = s1b[0]
    for n in range(1, 8):
        row = row + s1b[n]
    s2b[q * 4 + y] = row
    squares_2 = stage("s2", [(s2b.at[q * 4 + y], s2b.at[q * 4 + y], to) for to in around], s2b.at[pl.ds(0, 15)])
    with jax.named_scope("w_c0"):
        spread[0].wait_recv()
    start_tp(lax.rem(zp(2), 4))
    w_near = stage("wn", [(wb.at[:, q], wb.at[:, q], at_z(d)) for d in (14, 1, 15)], wb.at[pl.ds(0, 3)])

    with jax.named_scope("w_bg_y"):
        m_tp.wait_recv()
    with jax.named_scope("w_s2"):
        squares_2.wait_recv()
    with jax.named_scope("w_y"):
        across.wait_recv()

    total_sq = jnp.sum(jnp.sum(s2b[...], axis=0), axis=1, keepdims=True)
    clip_limit = clip_target * jnp.sqrt(jnp.float32(2 * D * RANK))
    clip_factor = jnp.minimum(1.0, clip_limit / jnp.sqrt(total_sq + norm_eps))

    left, right = at_x(3), at_x(1)
    xc_left, xc_right, xc_across = xp(3) * 2 + c, xp(1) * 2 + c, xp(2) * 2 + c
    piece = wb.at[pl.ds(0, 2)]

    def pair(half, which, n, to):
        for ref in (ko_ref, vo_ref):
            at = ref.at[pl.ds(half * 8, 8), which]
            remote(at, at, o_s.at[n], o_r.at[n], to).start()
        return remote(piece, piece, o_s.at[n], o_r.at[n], to)

    def to_partner(half, which):
        for ref in (ko_ref, vo_ref):
            at = ref.at[pl.ds(half * 8, 8), which]
            remote(at, at, o_s.at[6], o_r.at[6], partner).start()

    go_right, go_left = [], []
    for half in range(2):
        pieces = []
        for t in range(NY):
            at = pl.ds(half * 2, 2)
            scaled = clip_factor * gy[t, at].astype(f32).reshape(64, 128)
            first_new = beta_first * mb[t, at, :, 0].reshape(64, 128) + (1.0 - beta_first) * scaled
            second_new = beta_second * mb[t, at, :, 1].reshape(64, 128) + (1.0 - beta_second) * scaled * scaled
            firsts[t, pl.ds(half * 8, 8)] = first_new.reshape(8, 8, 128)
            seconds[t, pl.ds(half * 8, 8)] = second_new.reshape(8, 8, 128)
            pieces.append(first_new / (jnp.sqrt(second_new) + small_eps))
        direction = jnp.concatenate(pieces, axis=1)
        upper = direction.astype(bf16)
        lower = (direction - upper.astype(f32)).astype(bf16)
        product = lax.dot_general(
            jnp.concatenate([upper, lower], axis=0), wt[...], (((1,), (1,)), ((), ())), preferred_element_type=f32
        )
        product = product[0:64] + product[64:128]
        upd[pl.ds(half * 8, 8)] = product.reshape(8, 8, 2 * NW)
        if half == 0:
            with jax.named_scope("w_bg_wn"):
                w_near.wait_recv()
        old = wb[pl.ds(half * 2, 2)].reshape(8, 16, NW).astype(f32)
        moved = jnp.stack(
            [product[:, 0:NW].reshape(8, 8, NW), product[:, NW : 2 * NW].reshape(8, 8, NW)], axis=1
        ).reshape(8, 16, NW)
        new = (old - step_rate * moved).astype(bf16)
        ko_ref[pl.ds(half * 8, 8), xc] = new[:, :, 0:NK]
        vo_ref[pl.ds(half * 8, 8), xc] = new[:, :, NK:NW]
        if half == 0:
            go_right.append(pair(0, xc, 0, right))
            to_partner(0, xc)
        else:
            go_left.append(pair(1, xc, 3, left))
            go_right.append(pair(1, xc, 1, right))
            go_left.append(pair(0, xc, 4, left))
            to_partner(1, xc)

    for out, packed_all in ((first_ref, firsts), (second_ref, seconds)):
        packed = packed_all[y, z]
        out[0, 0:8, :] = packed[:, 0:32]
        out[1, 0:8, :] = packed[:, 32:64]
        out[0, 8:16, :] = packed[:, 64:96]
        out[1, 8:16, :] = packed[:, 96:128]
    own_upd = upd[z]
    for half in range(2):
        rows = slice(half * 8, half * 8 + 8)
        at = half * NW
        nk_ref[rows, :] = kvw[rows, 0:NK] - step_rate * own_upd[:, at : at + NK]
        nv_ref[rows, :] = kvw[rows, NK:NW] - step_rate * own_upd[:, at + NK : at + NW]

    finish.append(near)
    finish.append(across)
    for copy in to_core + to_x + finish:
        copy.wait_send()
    remote(arecv, arecv, send_sem["g"], g_r.at[0], partner).wait_send()

    with jax.named_scope("w_o0"):
        go_right[0].wait_recv()
    go_right.append(pair(0, xc_left, 2, right))
    to_partner(0, xc_left)
    with jax.named_scope("w_o1"):
        go_left[0].wait_recv()
    go_left.append(pair(1, xc_right, 5, left))
    to_partner(1, xc_right)
    with jax.named_scope("w_o2"):
        go_right[1].wait_recv()
    to_partner(1, xc_left)
    with jax.named_scope("w_o3"):
        go_left[1].wait_recv()
    to_partner(0, xc_right)
    with jax.named_scope("w_o4"):
        go_right[2].wait_recv()
    to_partner(0, xc_across)
    with jax.named_scope("w_o5"):
        go_left[2].wait_recv()
    to_partner(1, xc_across)
    with jax.named_scope("w_osend"):
        for copy in go_right + go_left:
            copy.wait_send()
    with jax.named_scope("w_oc"):
        both_ways = vo_ref.at[pl.ds(0, 12)]
        last = remote(both_ways, both_ways, o_s.at[6], o_r.at[6], partner)
        last.wait_recv()
        last.wait_send()


def store(*refs):
    sems = refs[-1]
    count = (len(refs) - 1) // 2
    copies = [pltpu.make_async_copy(refs[n], refs[count + n], sems.at[n]) for n in range(count)]
    for copy in reversed(copies):
        copy.start()
    for copy in copies:
        copy.wait()


def local(*args):
    vmem = pl.BlockSpec(memory_space=pltpu.VMEM)
    hbm = pl.BlockSpec(memory_space=pltpu.HBM)
    dma = pltpu.SemaphoreType.DMA
    shape = jax.ShapeDtypeStruct
    outs = pl.pallas_call(
        kernel,
        out_shape=(
            shape((2, 16, 32), f32),
            shape((2, 16, 32), f32),
            shape((16, NK), f32),
            shape((16, NV), f32),
            shape((NZ, NX * NC, 16, NK), bf16),
            shape((NZ, NX * NC, 16, NV), bf16),
        ),
        in_specs=[hbm] * 9,
        out_specs=[vmem] * 6,
        scratch_shapes=[
            pltpu.VMEM((TOK, D), bf16),
            pltpu.VMEM((D, TOK), bf16),
            pltpu.VMEM((TOK, NW), bf16),
            pltpu.VMEM((NW, RANK), bf16),
            pltpu.VMEM((16, NW), f32),
            pltpu.VMEM((2, 2, 16, 32), f32),
            pltpu.VMEM((2 * NW, 4 * 128), bf16),
            pltpu.VMEM((NY, HALF, 128), bf16),
            pltpu.VMEM((NY - 1, HALF, 128), bf16),
            pltpu.VMEM((4, NX, NC, 32, 128), bf16),
            pltpu.VMEM((4, NX, 32, 128), bf16),
            pltpu.VMEM((4, NX, 32, 128), bf16),
            pltpu.VMEM((4, NX - 1, 32, 128), bf16),
            pltpu.VMEM((3, 32, 128), bf16),
            pltpu.VMEM((3, 32, 128), bf16),
            pltpu.VMEM((4, 32, 128), bf16),
            pltpu.VMEM((NY, 4, 32, 128), bf16),
            pltpu.VMEM((NY, 4, 4, 2, 8, 128), f32),
            pltpu.VMEM((4, 4, 16, NW), bf16),
            pltpu.VMEM((NX * NC, 1, 128), f32),
            pltpu.VMEM((4 * NY, 1, 128), f32),
            pltpu.VMEM((NY, 16, 8, 128), f32),
            pltpu.VMEM((NY, 16, 8, 128), f32),
            pltpu.VMEM((16, 8, 2 * NW), f32),
            dma((5,)), dma((4,)), dma((4,)), dma((4,)), dma((4,)), dma((3,)), dma((7,)), dma((7,)), dma((12,)), dma((12,)),
        ],
        compiler_params=pltpu.CompilerParams(
            collective_id=0, has_side_effects=True, vmem_limit_bytes=40 * 1024 * 1024
        ),
        name="step",
    )(*[pltpu.with_memory_space_constraint(a, pltpu.HBM) for a in args])
    results = (*outs[:4], outs[4].reshape(D, NK), outs[5].reshape(D, NV))
    return pl.pallas_call(
        store,
        out_shape=tuple(shape(r.shape, r.dtype) for r in results),
        in_specs=[pl.BlockSpec(memory_space=pl.ANY)] * 6,
        out_specs=[hbm] * 6,
        scratch_shapes=[dma((6,))],
        compiler_params=pltpu.CompilerParams(vmem_limit_bytes=1024 * 1024),
        name="store",
    )(*results)


def solution(mesh):
    torus = Mesh(mesh.devices.reshape(NZ, NX, NC, NY), ("z", "x", "c", "y"))
    return jax.shard_map(
        local,
        mesh=torus,
        in_specs=(
            P(FS, None), P(FS, "y"), P(FS, "y"), P("y", None), P("y", None), P(FS, "y"), P(FS, "y"),
            P(None, FS, "y"), P(None, FS, "y"),
        ),
        out_specs=(P(None, FS, "y"), P(None, FS, "y"), P(FS, "y"), P(FS, "y"), P(None, "y"), P(None, "y")),
        check_vma=False,
    )
```

```python
import jax
import jax.numpy as jnp
from jax import lax
from jax.experimental import pallas as pl
from jax.experimental.pallas import tpu as pltpu
from jax.sharding import Mesh
from jax.sharding import PartitionSpec as P

D = 2048
RANK = 128
NZ, NX, NC, NY = 16, 4, 2, 4
FS = ("z", "x", "c")
TOK = 640
HALF = TOK // 2
NK = 128
NV = 256
NW = NK + NV

step_rate = 0.05
clip_target = 0.1
beta_first = 0.8
beta_second = 0.95
small_eps = 1e-08
norm_eps = 1e-06

FAR = (4, 12, 8)
f32 = jnp.float32
bf16 = jnp.bfloat16


def kernel(
    x_hbm, ck_hbm, cv_hbm, fk_hbm, fv_hbm, kw_hbm, vw_hbm, m_hbm, v_hbm,
    first_ref, second_ref, nk_ref, nv_ref, ko_ref, vo_ref,
    x_vm, xt, ckv, fkv, kvw, mv, wt, msend, yrecv, asend, crecv, xsend, xrecv, tsend, arecv, brecv, gy, mb, wb, sb,
    firsts, seconds, upd,
    in_sem, c_s, c_r, x_s, x_r, g_r, o_s, o_r, one_s, one_r,
):
    z, x, c, y = (lax.axis_index(n) for n in ("z", "x", "c", "y"))
    k, q = lax.div(z, 4), lax.rem(z, 4)
    other = 1 - c
    xc = x * 2 + c

    def zp(d):
        return lax.rem(z + d, NZ)

    def xp(d):
        return lax.rem(x + d, NX)

    def yp(d):
        return lax.rem(y + d, NY)

    def at_z(d):
        return (zp(d), x, c, y)

    def at_x(d):
        return (z, xp(d), c, y)

    def at_y(d):
        return (z, x, c, yp(d))

    partner = (z, x, other, y)

    def remote(src, dst, send, recv, to):
        return pltpu.make_async_remote_copy(
            src_ref=src, dst_ref=dst, send_sem=send, recv_sem=recv,
            device_id=to, device_id_type=pl.DeviceIdType.MESH,
        )

    names = ("tp", "a", "b", "g", "h", "sq", "mf", "mn", "my", "wf", "wn")
    send_sem = {name: one_s.at[n] for n, name in enumerate(names)}
    recv_sem = {name: one_r.at[n] for n, name in enumerate(names)}
    finish = []

    def stage(name, copies, whole):
        made = [remote(src, dst, send_sem[name], recv_sem[name], to) for src, dst, to in copies]
        for copy in made:
            copy.start()
        total = remote(whole, whole, send_sem[name], recv_sem[name], partner)
        finish.append(total)
        return total

    load_f = [pltpu.make_async_copy(fk_hbm, fkv.at[pl.ds(0, NK)], in_sem.at[0]),
              pltpu.make_async_copy(fv_hbm, fkv.at[pl.ds(NK, NV)], in_sem.at[0])]
    load_c = [pltpu.make_async_copy(ck_hbm, ckv.at[:, pl.ds(0, NK)], in_sem.at[1]),
              pltpu.make_async_copy(cv_hbm, ckv.at[:, pl.ds(NK, NV)], in_sem.at[1])]
    load_x = pltpu.make_async_copy(x_hbm, x_vm, in_sem.at[2])
    load_m = [pltpu.make_async_copy(m_hbm, mv.at[0], in_sem.at[3]),
              pltpu.make_async_copy(v_hbm, mv.at[1], in_sem.at[3])]
    load_w = [pltpu.make_async_copy(kw_hbm, kvw.at[:, pl.ds(0, NK)], in_sem.at[4]),
              pltpu.make_async_copy(vw_hbm, kvw.at[:, pl.ds(NK, NV)], in_sem.at[4])]

    for load in load_f + load_c:
        load.start()
    sources = [at_z(d) for d in FAR + (2, 15, 1)] + [at_y(d) for d in (2, 1, 3)] + [at_x(d) for d in (2, 1, 3)] + [partner]
    barrier = pltpu.get_barrier_semaphore()
    for peer in sources:
        pl.semaphore_signal(barrier, inc=1, device_id=peer, device_id_type=pl.DeviceIdType.MESH)
    for load in load_m + load_w + [load_x]:
        load.start()

    with jax.named_scope("w_factor"):
        pltpu.make_async_copy(fkv, fkv, in_sem.at[0]).wait()
    factor = fkv[...].astype(f32)
    rolled = [factor if s == 0 else pltpu.roll(factor, 32 * s, 1) for s in range(4)]
    lane_group = lax.broadcasted_iota(jnp.int32, (NW, 128), 1) // 32
    is_value = (lax.broadcasted_iota(jnp.int32, (NW, 128), 0) >= NK).astype(jnp.int32)
    for half in range(2):
        keep = lane_group == 2 * half + is_value
        for t in range(NY):
            at = (2 * half - t) % 4
            placed = jnp.concatenate([rolled[at][0:NK], rolled[(at + 1) % 4][NK:NW]], axis=0)
            wt[pl.ds(half * NW, NW), pl.ds(t * 128, 128)] = jnp.where(keep, placed, 0.0).astype(bf16)

    with jax.named_scope("w_cot"):
        pltpu.make_async_copy(ckv, ckv, in_sem.at[1]).wait()
    lhs = jnp.concatenate([ckv[0:HALF], ckv[HALF:TOK]], axis=1)
    reduced = jnp.dot(lhs, wt[...], preferred_element_type=f32)
    for t in range(NY):
        msend[t] = reduced[:, t * 128 : (t + 1) * 128].astype(bf16)

    pltpu.make_async_copy(mv, mv, in_sem.at[3]).wait()
    pltpu.make_async_copy(kvw, kvw, in_sem.at[4]).wait()
    for n in range(2):
        mb[y, k, q, n] = jnp.concatenate(
            [mv[n, 0, 0:8, :], mv[n, 1, 0:8, :], mv[n, 0, 8:16, :], mv[n, 1, 8:16, :]], axis=1
        )
    wb[k, q] = kvw[...].astype(bf16)

    with jax.named_scope("w_barrier"):
        pl.semaphore_wait(barrier, len(sources))

    tp = stage("tp", [(msend.at[yp(d)], yrecv.at[d - 1], at_y(d)) for d in (2, 1, 3)], yrecv)
    m_far = stage("mf", [(mb.at[y, k, q], mb.at[y, k, q], at_z(d)) for d in (8, 4, 12)], mb.at[0, 0, pl.ds(0, 3)])
    w_far = stage("wf", [(wb.at[k, q], wb.at[k, q], at_z(d)) for d in (8, 4, 12)], wb.at[0, pl.ds(0, 3)])

    load_x.wait()
    for n in range(8):
        xt[pl.ds(n * 256, 256), :] = x_vm[:, n * 256 : (n + 1) * 256].T

    with jax.named_scope("w_tp"):
        tp.wait_recv()
    own = msend[y].astype(f32)
    for n in range(3):
        own = own + yrecv[n].astype(f32)
    swapped = pltpu.roll(own, 64, 1)
    low = lax.broadcasted_iota(jnp.int32, (HALF, 128), 1) < 64
    both = jnp.concatenate([jnp.where(low, own, swapped), jnp.where(low, swapped, own)], axis=0)
    upper = both.astype(bf16)
    lower = (both - upper.astype(f32)).astype(bf16)
    rhs = jnp.concatenate([upper, lower], axis=1)
    low_tile = lax.broadcasted_iota(jnp.int32, (16, 8, 128), 2) < 64

    order = (14, 1, 15, 0)
    quarters = [lax.rem(zp(d), 4) for d in order]

    def product_of(n):
        for half in range(2):
            rows = pl.ds(pl.multiple_of(quarters[n] * 512 + half * 256, 256), 256)
            wide = jnp.dot(xt[rows, :], rhs, preferred_element_type=f32)
            part = (wide[:, :128] + wide[:, 128:]).reshape(16, 2, 8, 128)
            packed = jnp.where(low_tile, part[:, 0], part[:, 1]).reshape(2, 8, 8, 128)
            for t in range(8):
                asend[n, t // 2, t % 2, pl.ds(half * 16, 16), :] = packed[:, t].reshape(16, 128).astype(bf16)
        copy = remote(asend.at[n, :, other], crecv.at[n], c_s.at[n], c_r.at[n], partner)
        copy.start()
        return copy

    to_core, to_x = [], []

    def core_to_x(n):
        with jax.named_scope(f"w_core{n}"):
            to_core[n].wait_recv()
        for t in range(NX):
            xsend[n, t] = (asend[n, t, c].astype(f32) + crecv[n, t].astype(f32)).astype(bf16)
        for d in (2, 1, 3):
            remote(xsend.at[n, xp(d)], xrecv.at[n, d - 1], x_s.at[n], x_r.at[n], at_x(d)).start()
        to_x.append(remote(xrecv.at[n], xrecv.at[n], x_s.at[n], x_r.at[n], partner))

    to_core.append(product_of(0))
    for n in range(1, 4):
        to_core.append(product_of(n))
        core_to_x(n - 1)
    core_to_x(3)

    with jax.named_scope("w_bg_far"):
        m_far.wait_recv()
    m_near = stage("mn", [(mb.at[y, :, q], mb.at[y, :, q], at_z(d)) for d in (14, 1, 15)], mb.at[0, pl.ds(0, 3)])

    near = []
    for n in range(4):
        with jax.named_scope(f"w_x{n}"):
            to_x[n].wait_recv()
        total = xsend[n, x].astype(f32)
        for i in range(3):
            total = total + xrecv[n, i].astype(f32)
        if n < 3:
            tsend[n] = total.astype(bf16)
            remote(tsend.at[n], arecv.at[n], send_sem["a"], recv_sem["a"], at_z(order[n])).start()
    near = remote(arecv, arecv, send_sem["a"], recv_sem["a"], partner)

    with jax.named_scope("w_bg_near"):
        m_near.wait_recv()
    m_tp = stage("my", [(mb.at[y], mb.at[y], at_y(d)) for d in (2, 1, 3)], mb.at[pl.ds(0, 3)])

    with jax.named_scope("w_a"):
        near.wait_recv()
    for n in range(3):
        total = total + arecv[n].astype(f32)
    brecv[k] = total.astype(bf16)
    far = stage("b", [(brecv.at[k], brecv.at[k], at_z(d)) for d in (8, 4, 12)], brecv.at[pl.ds(0, 3)])
    with jax.named_scope("w_bg_wf"):
        w_far.wait_recv()
    with jax.named_scope("w_b"):
        far.wait_recv()
    total = brecv[0].astype(f32)
    for n in range(1, 4):
        total = total + brecv[n].astype(f32)
    rounded = total.astype(bf16)
    gy[y, q] = rounded
    rounded = rounded.astype(f32)

    def spot(residue, yy, which):
        return (residue * NY + yy) * (NX * NC) + which

    mine = sb.at[spot(q, y, xc)]
    mine[...] = jnp.sum(rounded * rounded, axis=0, keepdims=True)
    around = sorted(
        ((dz, dx, dc, dy) for dz in (14, 15, 1, 0) for dx in range(NX) for dc in range(NC) for dy in range(NY)),
        key=lambda d: -(min(d[0], NZ - d[0]) + min(d[1], NX - d[1]) + min(d[3], NY - d[3]) + d[2] * 0.5),
    )[:-1]

    def to_tp(part):
        return [(gy.at[y, part], gy.at[y, part], at_y(d)) for d in (2, 1, 3)]

    def start_tp(part):
        for src, dst, to in to_tp(part):
            remote(src, dst, send_sem["h"], recv_sem["h"], to).start()

    spread = [remote(gy.at[y, q], gy.at[y, q], send_sem["g"], g_r.at[n], at_z(d)) for n, d in enumerate((14, 1, 15))]
    for copy in spread:
        copy.start()
    start_tp(q)
    across = remote(gy.at[pl.ds(0, 3)], gy.at[pl.ds(0, 3)], send_sem["h"], recv_sem["h"], partner)
    squares = stage(
        "sq",
        [(mine, mine, (zp(dz), xp(dx), c if dc == 0 else other, yp(dy))) for dz, dx, dc, dy in around],
        sb.at[pl.ds(0, len(around))],
    )
    for n, d in ((1, 15), (2, 1)):
        with jax.named_scope(f"w_c{n}"):
            spread[n].wait_recv()
        start_tp(lax.rem(zp(d), 4))
    with jax.named_scope("w_c0"):
        spread[0].wait_recv()
    start_tp(lax.rem(zp(2), 4))
    w_near = stage("wn", [(wb.at[:, q], wb.at[:, q], at_z(d)) for d in (14, 1, 15)], wb.at[pl.ds(0, 3)])

    with jax.named_scope("w_bg_y"):
        m_tp.wait_recv()
    with jax.named_scope("w_y"):
        across.wait_recv()
    with jax.named_scope("w_s"):
        squares.wait_recv()

    total_sq = jnp.sum(jnp.sum(sb[...], axis=0), axis=1, keepdims=True)
    clip_limit = clip_target * jnp.sqrt(jnp.float32(2 * D * RANK))
    clip_factor = jnp.minimum(1.0, clip_limit / jnp.sqrt(total_sq + norm_eps))

    left, right = at_x(3), at_x(1)
    xc_left, xc_right, xc_across = xp(3) * 2 + c, xp(1) * 2 + c, xp(2) * 2 + c
    piece = wb.at[0]

    def send_piece(part, which, send, recv, to):
        for ref in (ko_ref, vo_ref):
            at = ref.at[pl.ds(part * 4, 4), which]
            remote(at, at, send, recv, to).start()

    go_right, go_left = [], []

    def to_right(part, which):
        n = len(go_right)
        send_piece(part, which, o_s.at[n], o_r.at[n], right)
        go_right.append(remote(piece, piece, o_s.at[n], o_r.at[n], right))

    def to_left(part, which):
        n = 6 + len(go_left)
        send_piece(part, which, o_s.at[n], o_r.at[n], left)
        go_left.append(remote(piece, piece, o_s.at[n], o_r.at[n], left))

    def to_partner(part, which):
        send_piece(part, which, o_s.at[12], o_r.at[12], partner)

    for part in (0, 3, 1, 2):
        pieces = []
        for t in range(NY):
            scaled = clip_factor * gy[t, part].astype(f32)
            first_new = beta_first * mb[t, part, :, 0].reshape(32, 128) + (1.0 - beta_first) * scaled
            second_new = beta_second * mb[t, part, :, 1].reshape(32, 128) + (1.0 - beta_second) * scaled * scaled
            firsts[t, pl.ds(part * 4, 4)] = first_new.reshape(4, 8, 128)
            seconds[t, pl.ds(part * 4, 4)] = second_new.reshape(4, 8, 128)
            pieces.append(first_new / (jnp.sqrt(second_new) + small_eps))
        direction = jnp.concatenate(pieces, axis=1)
        upper = direction.astype(bf16)
        lower = (direction - upper.astype(f32)).astype(bf16)
        product = lax.dot_general(
            jnp.concatenate([upper, lower], axis=0), wt[...], (((1,), (1,)), ((), ())), preferred_element_type=f32
        )
        product = product[0:32] + product[32:64]
        upd[pl.ds(part * 4, 4)] = product.reshape(4, 8, 2 * NW)
        if part == 0:
            with jax.named_scope("w_bg_wn"):
                w_near.wait_recv()
        old = wb[part].astype(f32)
        moved = jnp.stack(
            [product[:, 0:NW].reshape(4, 8, NW), product[:, NW : 2 * NW].reshape(4, 8, NW)], axis=1
        ).reshape(4, 16, NW)
        new = (old - step_rate * moved).astype(bf16)
        ko_ref[pl.ds(part * 4, 4), xc] = new[:, :, 0:NK]
        vo_ref[pl.ds(part * 4, 4), xc] = new[:, :, NK:NW]
        if part != 3:
            to_right(part, xc)
        if part >= 2:
            to_left(part, xc)
        to_partner(part, xc)
    to_left(1, xc)
    to_right(3, xc)
    to_left(0, xc)

    for out, packed_all in ((first_ref, firsts), (second_ref, seconds)):
        packed = packed_all[y, z]
        out[0, 0:8, :] = packed[:, 0:32]
        out[1, 0:8, :] = packed[:, 32:64]
        out[0, 8:16, :] = packed[:, 64:96]
        out[1, 8:16, :] = packed[:, 96:128]
    own_upd = upd[z]
    for half in range(2):
        rows = slice(half * 8, half * 8 + 8)
        at = half * NW
        nk_ref[rows, :] = kvw[rows, 0:NK] - step_rate * own_upd[:, at : at + NK]
        nv_ref[rows, :] = kvw[rows, NK:NW] - step_rate * own_upd[:, at + NK : at + NW]

    finish.append(near)
    finish.append(across)
    for copy in to_core + to_x + finish:
        copy.wait_send()
    remote(arecv, arecv, send_sem["g"], g_r.at[0], partner).wait_send()

    for n in range(6):
        with jax.named_scope(f"w_r{n}"):
            go_right[n].wait_recv()
        if n < 2:
            to_right(n, xc_left)
        to_partner(n % 4, xc_left if n < 4 else xc_across)
        with jax.named_scope(f"w_l{n}"):
            go_left[n].wait_recv()
        if n < 2:
            to_left(3 - n, xc_right)
        to_partner(3 - n % 4, xc_right if n < 4 else xc_across)
    with jax.named_scope("w_osend"):
        for copy in go_right + go_left:
            copy.wait_send()
    with jax.named_scope("w_oc"):
        both_ways = vo_ref.at[pl.ds(0, 12)]
        last = remote(both_ways, both_ways, o_s.at[12], o_r.at[12], partner)
        last.wait_recv()
        last.wait_send()


def store(*refs):
    sems = refs[-1]
    count = (len(refs) - 1) // 2
    copies = [pltpu.make_async_copy(refs[n], refs[count + n], sems.at[n]) for n in range(count)]
    for copy in reversed(copies):
        copy.start()
    for copy in copies:
        copy.wait()


def local(*args):
    vmem = pl.BlockSpec(memory_space=pltpu.VMEM)
    hbm = pl.BlockSpec(memory_space=pltpu.HBM)
    dma = pltpu.SemaphoreType.DMA
    shape = jax.ShapeDtypeStruct
    outs = pl.pallas_call(
        kernel,
        out_shape=(
            shape((2, 16, 32), f32),
            shape((2, 16, 32), f32),
            shape((16, NK), f32),
            shape((16, NV), f32),
            shape((NZ, NX * NC, 16, NK), bf16),
            shape((NZ, NX * NC, 16, NV), bf16),
        ),
        in_specs=[hbm] * 9,
        out_specs=[vmem] * 6,
        scratch_shapes=[
            pltpu.VMEM((TOK, D), bf16),
            pltpu.VMEM((D, TOK), bf16),
            pltpu.VMEM((TOK, NW), bf16),
            pltpu.VMEM((NW, RANK), bf16),
            pltpu.VMEM((16, NW), f32),
            pltpu.VMEM((2, 2, 16, 32), f32),
            pltpu.VMEM((2 * NW, 4 * 128), bf16),
            pltpu.VMEM((NY, HALF, 128), bf16),
            pltpu.VMEM((NY - 1, HALF, 128), bf16),
            pltpu.VMEM((4, NX, NC, 32, 128), bf16),
            pltpu.VMEM((4, NX, 32, 128), bf16),
            pltpu.VMEM((4, NX, 32, 128), bf16),
            pltpu.VMEM((4, NX - 1, 32, 128), bf16),
            pltpu.VMEM((3, 32, 128), bf16),
            pltpu.VMEM((3, 32, 128), bf16),
            pltpu.VMEM((4, 32, 128), bf16),
            pltpu.VMEM((NY, 4, 32, 128), bf16),
            pltpu.VMEM((NY, 4, 4, 2, 8, 128), f32),
            pltpu.VMEM((4, 4, 16, NW), bf16),
            pltpu.VMEM((4 * NY * NX * NC, 1, 128), f32),
            pltpu.VMEM((NY, 16, 8, 128), f32),
            pltpu.VMEM((NY, 16, 8, 128), f32),
            pltpu.VMEM((16, 8, 2 * NW), f32),
            dma((5,)), dma((4,)), dma((4,)), dma((4,)), dma((4,)), dma((3,)), dma((13,)), dma((13,)), dma((11,)), dma((11,)),
        ],
        compiler_params=pltpu.CompilerParams(
            collective_id=0, has_side_effects=True, vmem_limit_bytes=40 * 1024 * 1024
        ),
        name="step",
    )(*[pltpu.with_memory_space_constraint(a, pltpu.HBM) for a in args])
    results = (*outs[:4], outs[4].reshape(D, NK), outs[5].reshape(D, NV))
    return pl.pallas_call(
        store,
        out_shape=tuple(shape(r.shape, r.dtype) for r in results),
        in_specs=[pl.BlockSpec(memory_space=pl.ANY)] * 6,
        out_specs=[hbm] * 6,
        scratch_shapes=[dma((6,))],
        compiler_params=pltpu.CompilerParams(vmem_limit_bytes=1024 * 1024),
        name="store",
    )(*results)


def solution(mesh):
    torus = Mesh(mesh.devices.reshape(NZ, NX, NC, NY), ("z", "x", "c", "y"))
    return jax.shard_map(
        local,
        mesh=torus,
        in_specs=(
            P(FS, None), P(FS, "y"), P(FS, "y"), P("y", None), P("y", None), P(FS, "y"), P(FS, "y"),
            P(None, FS, "y"), P(None, FS, "y"),
        ),
        out_specs=(P(None, FS, "y"), P(None, FS, "y"), P(FS, "y"), P(FS, "y"), P(None, "y"), P(None, "y")),
        check_vma=False,
    )
```

```python
import jax
import jax.numpy as jnp
from jax import lax
from jax.experimental import pallas as pl
from jax.experimental.pallas import tpu as pltpu
from jax.sharding import Mesh
from jax.sharding import PartitionSpec as P

D = 2048
RANK = 128
NZ, NX, NC, NY = 16, 4, 2, 4
FS = ("z", "x", "c")
TOK = 640
HALF = TOK // 2
NK = 128
NV = 256
NW = NK + NV

step_rate = 0.05
clip_target = 0.1
beta_first = 0.8
beta_second = 0.95
small_eps = 1e-08
norm_eps = 1e-06

FAR = (4, 12, 8)
f32 = jnp.float32
bf16 = jnp.bfloat16


def kernel(
    x_hbm, ck_hbm, cv_hbm, fk_hbm, fv_hbm, kw_hbm, vw_hbm, m_hbm, v_hbm,
    first_ref, second_ref, nk_ref, nv_ref, ko_ref, vo_ref,
    x_vm, ckv, fkv, kvw, mv, wt, wtt, msend, yrecv, asend, crecv, xsend, xrecv, tsend, arecv, brecv, gy, mb, wb, sb,
    firsts, seconds, upd,
    in_sem, c_s, c_r, x_s, x_r, o_s, o_r, one_s, one_r,
):
    z, x, c, y = (lax.axis_index(n) for n in ("z", "x", "c", "y"))
    k, q = lax.div(z, 4), lax.rem(z, 4)
    other = 1 - c
    xc = x * 2 + c

    def zp(d):
        return lax.rem(z + d, NZ)

    def xp(d):
        return lax.rem(x + d, NX)

    def yp(d):
        return lax.rem(y + d, NY)

    def at_z(d):
        return (zp(d), x, c, y)

    def at_x(d):
        return (z, xp(d), c, y)

    def at_y(d):
        return (z, x, c, yp(d))

    partner = (z, x, other, y)

    def remote(src, dst, send, recv, to):
        return pltpu.make_async_remote_copy(
            src_ref=src, dst_ref=dst, send_sem=send, recv_sem=recv,
            device_id=to, device_id_type=pl.DeviceIdType.MESH,
        )

    names = ("tp", "a", "b", "g", "h", "sq", "mf", "mn", "my", "wf", "wn")
    send_sem = {name: one_s.at[n] for n, name in enumerate(names)}
    recv_sem = {name: one_r.at[n] for n, name in enumerate(names)}
    finish = []

    def stage(name, copies, whole):
        made = [remote(src, dst, send_sem[name], recv_sem[name], to) for src, dst, to in copies]
        for copy in made:
            copy.start()
        total = remote(whole, whole, send_sem[name], recv_sem[name], partner)
        finish.append(total)
        return total

    load_f = [pltpu.make_async_copy(fk_hbm, fkv.at[pl.ds(0, NK)], in_sem.at[0]),
              pltpu.make_async_copy(fv_hbm, fkv.at[pl.ds(NK, NV)], in_sem.at[0])]
    load_c = [pltpu.make_async_copy(ck_hbm, ckv.at[:, pl.ds(0, NK)], in_sem.at[1]),
              pltpu.make_async_copy(cv_hbm, ckv.at[:, pl.ds(NK, NV)], in_sem.at[1])]
    load_x = pltpu.make_async_copy(x_hbm, x_vm, in_sem.at[2])
    load_m = [pltpu.make_async_copy(m_hbm, mv.at[0], in_sem.at[3]),
              pltpu.make_async_copy(v_hbm, mv.at[1], in_sem.at[3])]
    load_w = [pltpu.make_async_copy(kw_hbm, kvw.at[:, pl.ds(0, NK)], in_sem.at[4]),
              pltpu.make_async_copy(vw_hbm, kvw.at[:, pl.ds(NK, NV)], in_sem.at[4])]

    for load in load_f + load_c:
        load.start()
    sources = [at_z(d) for d in FAR + (2, 15, 1)] + [at_y(d) for d in (2, 1, 3)] + [at_x(d) for d in (2, 1, 3)] + [partner]
    barrier = pltpu.get_barrier_semaphore()
    for peer in sources:
        pl.semaphore_signal(barrier, inc=1, device_id=peer, device_id_type=pl.DeviceIdType.MESH)
    for load in load_m + load_w + [load_x]:
        load.start()

    with jax.named_scope("w_factor"):
        pltpu.make_async_copy(fkv, fkv, in_sem.at[0]).wait()
    factor = fkv[...].astype(f32)
    rolled = [factor if s == 0 else pltpu.roll(factor, 32 * s, 1) for s in range(4)]
    lane_group = lax.broadcasted_iota(jnp.int32, (NW, 128), 1) // 32
    is_value = (lax.broadcasted_iota(jnp.int32, (NW, 128), 0) >= NK).astype(jnp.int32)
    for half in range(2):
        keep = lane_group == 2 * half + is_value
        for t in range(NY):
            at = (2 * half - t) % 4
            placed = jnp.concatenate([rolled[at][0:NK], rolled[(at + 1) % 4][NK:NW]], axis=0)
            wt[pl.ds(half * NW, NW), pl.ds(t * 128, 128)] = jnp.where(keep, placed, 0.0).astype(bf16)

    with jax.named_scope("w_cot"):
        pltpu.make_async_copy(ckv, ckv, in_sem.at[1]).wait()
    lhs = jnp.concatenate([ckv[0:HALF], ckv[HALF:TOK]], axis=1)
    reduced = jnp.dot(lhs, wt[...], preferred_element_type=f32)
    for t in range(NY):
        msend[t] = reduced[:, t * 128 : (t + 1) * 128].astype(bf16)

    pltpu.make_async_copy(mv, mv, in_sem.at[3]).wait()
    pltpu.make_async_copy(kvw, kvw, in_sem.at[4]).wait()
    for n in range(2):
        mb[y, k, q, n] = jnp.concatenate(
            [mv[n, 0, 0:8, :], mv[n, 1, 0:8, :], mv[n, 0, 8:16, :], mv[n, 1, 8:16, :]], axis=1
        )
    wb[k, q] = kvw[...].astype(bf16)

    with jax.named_scope("w_barrier"):
        pl.semaphore_wait(barrier, len(sources))

    tp = stage("tp", [(msend.at[yp(d)], yrecv.at[d - 1], at_y(d)) for d in (2, 1, 3)], yrecv)
    m_far = stage("mf", [(mb.at[y, k, q], mb.at[y, k, q], at_z(d)) for d in (8, 4, 12)], mb.at[0, 0, pl.ds(0, 3)])
    w_far = stage("wf", [(wb.at[k, q], wb.at[k, q], at_z(d)) for d in (8, 4, 12)], wb.at[0, pl.ds(0, 3)])

    load_x.wait()
    for n in range(4):
        wtt[pl.ds(n * 128, 128), :] = wt[:, n * 128 : (n + 1) * 128].T

    with jax.named_scope("w_tp"):
        tp.wait_recv()
    own = msend[y].astype(f32)
    for n in range(3):
        own = own + yrecv[n].astype(f32)
    swapped = pltpu.roll(own, 64, 1)
    low = lax.broadcasted_iota(jnp.int32, (HALF, 128), 1) < 64
    both = jnp.concatenate([jnp.where(low, own, swapped), jnp.where(low, swapped, own)], axis=0)
    upper = both.astype(bf16).astype(f32)
    first_half = lax.broadcasted_iota(jnp.int32, (TOK, 128), 1) < 64
    stream = jnp.where(first_half, upper, both - upper).astype(bf16).T
    low_tile = lax.broadcasted_iota(jnp.int32, (32, 8, 128), 2) < 64

    order = (14, 1, 15, 0)
    quarters = [lax.rem(zp(d), 4) for d in order]

    def product_of(n):
        cols = pl.ds(pl.multiple_of(quarters[n] * 512, 512), 512)
        wide = jnp.dot(stream, x_vm[:, cols], preferred_element_type=f32)
        part = wide[0:64] + wide[64:128]
        part = jnp.concatenate([part, part], axis=0).T.reshape(32, 2, 8, 128)
        packed = jnp.where(low_tile, part[:, 0], part[:, 1]).reshape(4, 8, 8, 128)
        for t in range(8):
            asend[n, t // 2, t % 2] = packed[:, t].reshape(32, 128).astype(bf16)
        copy = remote(asend.at[n, :, other], crecv.at[n], c_s.at[n], c_r.at[n], partner)
        copy.start()
        return copy

    to_core, to_x = [], []

    def core_to_x(n):
        with jax.named_scope(f"w_core{n}"):
            to_core[n].wait_recv()
        for t in range(NX):
            xsend[n, t] = (asend[n, t, c].astype(f32) + crecv[n, t].astype(f32)).astype(bf16)
        for d in (2, 1, 3):
            remote(xsend.at[n, xp(d)], xrecv.at[n, d - 1], x_s.at[n], x_r.at[n], at_x(d)).start()
        to_x.append(remote(xrecv.at[n], xrecv.at[n], x_s.at[n], x_r.at[n], partner))

    for n in range(3):
        to_core.append(product_of(n))
    core_to_x(0)
    to_core.append(product_of(3))
    for n in range(1, 4):
        core_to_x(n)

    for n in range(4):
        with jax.named_scope(f"w_x{n}"):
            to_x[n].wait_recv()
        total = xsend[n, x].astype(f32)
        for i in range(3):
            total = total + xrecv[n, i].astype(f32)
        if n < 3:
            tsend[n] = total.astype(bf16)
            remote(tsend.at[n], arecv.at[n], send_sem["a"], recv_sem["a"], at_z(order[n])).start()
    near = remote(arecv, arecv, send_sem["a"], recv_sem["a"], partner)

    with jax.named_scope("w_bg_far"):
        m_far.wait_recv()
    m_near = stage("mn", [(mb.at[y, :, q], mb.at[y, :, q], at_z(d)) for d in (14, 1, 15)], mb.at[0, pl.ds(0, 3)])

    with jax.named_scope("w_a"):
        near.wait_recv()
    for n in range(3):
        total = total + arecv[n].astype(f32)
    brecv[k] = total.astype(bf16)
    far = stage("b", [(brecv.at[k], brecv.at[k], at_z(d)) for d in (8, 4, 12)], brecv.at[pl.ds(0, 3)])
    with jax.named_scope("w_bg_near"):
        m_near.wait_recv()
    m_tp = stage("my", [(mb.at[y], mb.at[y], at_y(d)) for d in (2, 1, 3)], mb.at[pl.ds(0, 3)])

    with jax.named_scope("w_bg_wf"):
        w_far.wait_recv()
    w_near = stage("wn", [(wb.at[:, q], wb.at[:, q], at_z(d)) for d in (14, 1, 15)], wb.at[pl.ds(0, 3)])
    with jax.named_scope("w_b"):
        far.wait_recv()
    total = brecv[0].astype(f32)
    for n in range(1, 4):
        total = total + brecv[n].astype(f32)
    rounded = total.astype(bf16)
    gy[y, q] = rounded
    rounded = rounded.astype(f32)

    def spot(residue, yy, which):
        return (residue * NY + yy) * (NX * NC) + which

    mine = sb.at[spot(q, y, xc)]
    mine[...] = jnp.sum(rounded * rounded, axis=0, keepdims=True)
    around = sorted(
        ((dz, dx, dc, dy) for dz in (14, 15, 1, 0) for dx in range(NX) for dc in range(NC) for dy in range(NY)),
        key=lambda d: -(min(d[0], NZ - d[0]) + min(d[1], NX - d[1]) + min(d[3], NY - d[3]) + d[2] * 0.5),
    )[:-1]

    def start_squares(some):
        for dz, dx, dc, dy in some:
            to = (zp(dz), xp(dx), c if dc == 0 else other, yp(dy))
            remote(mine, mine, send_sem["sq"], recv_sem["sq"], to).start()

    start_squares(around)
    part = gy.at[y, q]
    for dz in (14, 1, 15, 0):
        for dy in (2, 1, 3):
            remote(part, part, send_sem["h"], recv_sem["h"], (zp(dz), x, c, yp(dy))).start()
    spread = stage("g", [(part, part, at_z(d)) for d in (14, 1, 15)], arecv)
    across = remote(gy.at[pl.ds(0, 3)], gy.at[pl.ds(0, 3)], send_sem["h"], recv_sem["h"], partner)
    every = sb.at[pl.ds(0, len(around))]
    squares = remote(every, every, send_sem["sq"], recv_sem["sq"], partner)

    with jax.named_scope("w_bg_y"):
        m_tp.wait_recv()
    with jax.named_scope("w_c"):
        spread.wait_recv()
    with jax.named_scope("w_y"):
        across.wait_recv()
    with jax.named_scope("w_s"):
        squares.wait_recv()

    total_sq = jnp.sum(jnp.sum(sb[...], axis=0), axis=1, keepdims=True)
    clip_limit = clip_target * jnp.sqrt(jnp.float32(2 * D * RANK))
    clip_factor = jnp.minimum(1.0, clip_limit / jnp.sqrt(total_sq + norm_eps))

    left, right = at_x(3), at_x(1)
    xc_left, xc_right, xc_across = xp(3) * 2 + c, xp(1) * 2 + c, xp(2) * 2 + c
    piece = wb.at[0]

    def send_piece(part, which, send, recv, to):
        for ref in (ko_ref, vo_ref):
            at = ref.at[pl.ds(part * 4, 4), which]
            remote(at, at, send, recv, to).start()

    go_right, go_left = [], []

    def to_right(part, which):
        n = len(go_right)
        send_piece(part, which, o_s.at[n], o_r.at[n], right)
        go_right.append(remote(piece, piece, o_s.at[n], o_r.at[n], right))

    def to_left(part, which):
        n = 6 + len(go_left)
        send_piece(part, which, o_s.at[n], o_r.at[n], left)
        go_left.append(remote(piece, piece, o_s.at[n], o_r.at[n], left))

    def to_partner(part, which):
        send_piece(part, which, o_s.at[12], o_r.at[12], partner)

    for batch in ((0, 3), (1, 2)):
        rows = []
        for part in batch:
            pieces = []
            for t in range(NY):
                scaled = clip_factor * gy[t, part].astype(f32)
                first_new = beta_first * mb[t, part, :, 0].reshape(32, 128) + (1.0 - beta_first) * scaled
                second_new = beta_second * mb[t, part, :, 1].reshape(32, 128) + (1.0 - beta_second) * scaled * scaled
                firsts[t, pl.ds(part * 4, 4)] = first_new.reshape(4, 8, 128)
                seconds[t, pl.ds(part * 4, 4)] = second_new.reshape(4, 8, 128)
                pieces.append(first_new / (jnp.sqrt(second_new) + small_eps))
            rows.append(jnp.concatenate(pieces, axis=1))
        direction = jnp.concatenate(rows, axis=0)
        upper = direction.astype(bf16)
        lower = (direction - upper.astype(f32)).astype(bf16)
        product = jnp.dot(jnp.concatenate([upper, lower], axis=0), wtt[...], preferred_element_type=f32)
        product = product[0:64] + product[64:128]
        if batch[0] == 0:
            with jax.named_scope("w_bg_wn"):
                w_near.wait_recv()
        for n, part in enumerate(batch):
            change = product[n * 32 : n * 32 + 32]
            upd[pl.ds(part * 4, 4)] = change.reshape(4, 8, 2 * NW)
            moved = jnp.stack(
                [change[:, 0:NW].reshape(4, 8, NW), change[:, NW : 2 * NW].reshape(4, 8, NW)], axis=1
            ).reshape(4, 16, NW)
            new = (wb[part].astype(f32) - step_rate * moved).astype(bf16)
            ko_ref[pl.ds(part * 4, 4), xc] = new[:, :, 0:NK]
            vo_ref[pl.ds(part * 4, 4), xc] = new[:, :, NK:NW]
        if batch[0] == 0:
            to_right(0, xc)
            to_left(3, xc)
        else:
            to_right(1, xc)
            to_left(2, xc)
            to_right(2, xc)
            to_left(1, xc)
            to_right(3, xc)
            to_left(0, xc)
        for part in batch:
            to_partner(part, xc)

    for out, packed_all in ((first_ref, firsts), (second_ref, seconds)):
        packed = packed_all[y, z]
        out[0, 0:8, :] = packed[:, 0:32]
        out[1, 0:8, :] = packed[:, 32:64]
        out[0, 8:16, :] = packed[:, 64:96]
        out[1, 8:16, :] = packed[:, 96:128]
    own_upd = upd[z]
    for half in range(2):
        rows = slice(half * 8, half * 8 + 8)
        at = half * NW
        nk_ref[rows, :] = kvw[rows, 0:NK] - step_rate * own_upd[:, at : at + NK]
        nv_ref[rows, :] = kvw[rows, NK:NW] - step_rate * own_upd[:, at + NK : at + NW]

    finish.extend([near, across, squares])
    for copy in to_core + to_x + finish:
        copy.wait_send()

    for n in range(6):
        with jax.named_scope(f"w_r{n}"):
            go_right[n].wait_recv()
        if n < 2:
            to_right(n, xc_left)
        to_partner(n % 4, xc_left if n < 4 else xc_across)
        with jax.named_scope(f"w_l{n}"):
            go_left[n].wait_recv()
        if n < 2:
            to_left(3 - n, xc_right)
        to_partner(3 - n % 4, xc_right if n < 4 else xc_across)
    with jax.named_scope("w_osend"):
        for copy in go_right + go_left:
            copy.wait_send()
    with jax.named_scope("w_oc"):
        both_ways = vo_ref.at[pl.ds(0, 12)]
        last = remote(both_ways, both_ways, o_s.at[12], o_r.at[12], partner)
        last.wait_recv()
        last.wait_send()


def store(*refs):
    sems = refs[-1]
    count = (len(refs) - 1) // 2
    copies = [pltpu.make_async_copy(refs[n], refs[count + n], sems.at[n]) for n in range(count)]
    for copy in reversed(copies):
        copy.start()
    for copy in copies:
        copy.wait()


def local(*args):
    vmem = pl.BlockSpec(memory_space=pltpu.VMEM)
    hbm = pl.BlockSpec(memory_space=pltpu.HBM)
    dma = pltpu.SemaphoreType.DMA
    shape = jax.ShapeDtypeStruct
    outs = pl.pallas_call(
        kernel,
        out_shape=(
            shape((2, 16, 32), f32),
            shape((2, 16, 32), f32),
            shape((16, NK), f32),
            shape((16, NV), f32),
            shape((NZ, NX * NC, 16, NK), bf16),
            shape((NZ, NX * NC, 16, NV), bf16),
        ),
        in_specs=[hbm] * 9,
        out_specs=[vmem] * 6,
        scratch_shapes=[
            pltpu.VMEM((TOK, D), bf16),
            pltpu.VMEM((TOK, NW), bf16),
            pltpu.VMEM((NW, RANK), bf16),
            pltpu.VMEM((16, NW), f32),
            pltpu.VMEM((2, 2, 16, 32), f32),
            pltpu.VMEM((2 * NW, 4 * 128), bf16),
            pltpu.VMEM((4 * 128, 2 * NW), bf16),
            pltpu.VMEM((NY, HALF, 128), bf16),
            pltpu.VMEM((NY - 1, HALF, 128), bf16),
            pltpu.VMEM((4, NX, NC, 32, 128), bf16),
            pltpu.VMEM((4, NX, 32, 128), bf16),
            pltpu.VMEM((4, NX, 32, 128), bf16),
            pltpu.VMEM((4, NX - 1, 32, 128), bf16),
            pltpu.VMEM((3, 32, 128), bf16),
            pltpu.VMEM((3, 32, 128), bf16),
            pltpu.VMEM((4, 32, 128), bf16),
            pltpu.VMEM((NY, 4, 32, 128), bf16),
            pltpu.VMEM((NY, 4, 4, 2, 8, 128), f32),
            pltpu.VMEM((4, 4, 16, NW), bf16),
            pltpu.VMEM((4 * NY * NX * NC, 1, 128), f32),
            pltpu.VMEM((NY, 16, 8, 128), f32),
            pltpu.VMEM((NY, 16, 8, 128), f32),
            pltpu.VMEM((16, 8, 2 * NW), f32),
            dma((5,)), dma((4,)), dma((4,)), dma((4,)), dma((4,)), dma((13,)), dma((13,)), dma((11,)), dma((11,)),
        ],
        compiler_params=pltpu.CompilerParams(
            collective_id=0, has_side_effects=True, vmem_limit_bytes=40 * 1024 * 1024
        ),
        name="step",
    )(*[pltpu.with_memory_space_constraint(a, pltpu.HBM) for a in args])
    results = (*outs[:4], outs[4].reshape(D, NK), outs[5].reshape(D, NV))
    return pl.pallas_call(
        store,
        out_shape=tuple(shape(r.shape, r.dtype) for r in results),
        in_specs=[pl.BlockSpec(memory_space=pl.ANY)] * 6,
        out_specs=[hbm] * 6,
        scratch_shapes=[dma((6,))],
        compiler_params=pltpu.CompilerParams(vmem_limit_bytes=1024 * 1024),
        name="store",
    )(*results)


def solution(mesh):
    torus = Mesh(mesh.devices.reshape(NZ, NX, NC, NY), ("z", "x", "c", "y"))
    return jax.shard_map(
        local,
        mesh=torus,
        in_specs=(
            P(FS, None), P(FS, "y"), P(FS, "y"), P("y", None), P("y", None), P(FS, "y"), P(FS, "y"),
            P(None, FS, "y"), P(None, FS, "y"),
        ),
        out_specs=(P(None, FS, "y"), P(None, FS, "y"), P(FS, "y"), P(FS, "y"), P(None, "y"), P(None, "y")),
        check_vma=False,
    )
```

```python
import jax
import jax.numpy as jnp
from jax import lax
from jax.experimental import pallas as pl
from jax.experimental.pallas import tpu as pltpu
from jax.sharding import Mesh
from jax.sharding import PartitionSpec as P

D = 2048
RANK = 128
NZ, NX, NC, NY = 16, 4, 2, 4
FS = ("z", "x", "c")
TOK = 640
HALF = TOK // 2
NK = 128
NV = 256
NW = NK + NV

step_rate = 0.05
clip_target = 0.1
beta_first = 0.8
beta_second = 0.95
small_eps = 1e-08
norm_eps = 1e-06

FAR = (4, 12, 8)
f32 = jnp.float32
bf16 = jnp.bfloat16


def kernel(
    x_hbm, ck_hbm, cv_hbm, fk_hbm, fv_hbm, kw_hbm, vw_hbm, m_hbm, v_hbm,
    first_ref, second_ref, nk_ref, nv_ref, ko_ref, vo_ref,
    x_vm, ckv, fkv, kvw, mv, wt, wtt, msend, yrecv, asend, crecv, xsend, xrecv, tsend, arecv, brecv, gy, mb, wb, sb,
    firsts, seconds, upd,
    in_sem, ahead, c_s, c_r, x_s, x_r, o_s, o_r, one_s, one_r,
):
    z, x, c, y = (lax.axis_index(n) for n in ("z", "x", "c", "y"))
    k, q = lax.div(z, 4), lax.rem(z, 4)
    other = 1 - c
    xc = x * 2 + c

    def zp(d):
        return lax.rem(z + d, NZ)

    def xp(d):
        return lax.rem(x + d, NX)

    def yp(d):
        return lax.rem(y + d, NY)

    def at_z(d):
        return (zp(d), x, c, y)

    def at_x(d):
        return (z, xp(d), c, y)

    def at_y(d):
        return (z, x, c, yp(d))

    partner = (z, x, other, y)

    def remote(src, dst, send, recv, to):
        return pltpu.make_async_remote_copy(
            src_ref=src, dst_ref=dst, send_sem=send, recv_sem=recv,
            device_id=to, device_id_type=pl.DeviceIdType.MESH,
        )

    names = ("tp", "a", "b", "g", "h", "sq", "mf", "mn", "my", "wf", "wn")
    send_sem = {name: one_s.at[n] for n, name in enumerate(names)}
    recv_sem = {name: one_r.at[n] for n, name in enumerate(names)}
    finish = []

    def stage(name, copies, whole):
        made = [remote(src, dst, send_sem[name], recv_sem[name], to) for src, dst, to in copies]
        for copy in made:
            copy.start()
        total = remote(whole, whole, send_sem[name], recv_sem[name], partner)
        finish.append(total)
        return total

    load_f = [pltpu.make_async_copy(fk_hbm, fkv.at[pl.ds(0, NK)], in_sem.at[0]),
              pltpu.make_async_copy(fv_hbm, fkv.at[pl.ds(NK, NV)], in_sem.at[0])]
    load_c = [pltpu.make_async_copy(ck_hbm, ckv.at[:, pl.ds(0, NK)], in_sem.at[1]),
              pltpu.make_async_copy(cv_hbm, ckv.at[:, pl.ds(NK, NV)], in_sem.at[1])]
    load_x = pltpu.make_async_copy(x_hbm, x_vm, in_sem.at[2])
    load_m = [pltpu.make_async_copy(m_hbm, mv.at[0], in_sem.at[3]),
              pltpu.make_async_copy(v_hbm, mv.at[1], in_sem.at[3])]
    load_w = [pltpu.make_async_copy(kw_hbm, kvw.at[:, pl.ds(0, NK)], in_sem.at[4]),
              pltpu.make_async_copy(vw_hbm, kvw.at[:, pl.ds(NK, NV)], in_sem.at[4])]

    for load in load_f + load_c:
        load.start()
    sources = [at_z(d) for d in (2, 14, 15, 1)] + [at_y(d) for d in (2, 1, 3)] + [at_x(d) for d in (2, 1, 3)] + [partner]
    barrier = pltpu.get_barrier_semaphore()
    for peer in sources:
        pl.semaphore_signal(barrier, inc=1, device_id=peer, device_id_type=pl.DeviceIdType.MESH)
    for load in load_m + load_w + [load_x]:
        load.start()

    with jax.named_scope("w_factor"):
        pltpu.make_async_copy(fkv, fkv, in_sem.at[0]).wait()
    factor = fkv[...].astype(f32)
    rolled = [factor if s == 0 else pltpu.roll(factor, 32 * s, 1) for s in range(4)]
    lane_group = lax.broadcasted_iota(jnp.int32, (NW, 128), 1) // 32
    is_value = (lax.broadcasted_iota(jnp.int32, (NW, 128), 0) >= NK).astype(jnp.int32)
    for half in range(2):
        keep = lane_group == 2 * half + is_value
        for t in range(NY):
            at = (2 * half - t) % 4
            placed = jnp.concatenate([rolled[at][0:NK], rolled[(at + 1) % 4][NK:NW]], axis=0)
            wt[pl.ds(half * NW, NW), pl.ds(t * 128, 128)] = jnp.where(keep, placed, 0.0).astype(bf16)

    with jax.named_scope("w_cot"):
        pltpu.make_async_copy(ckv, ckv, in_sem.at[1]).wait()
    lhs = jnp.concatenate([ckv[0:HALF], ckv[HALF:TOK]], axis=1)
    reduced = jnp.dot(lhs, wt[...], preferred_element_type=f32)
    for t in range(NY):
        msend[t] = reduced[:, t * 128 : (t + 1) * 128].astype(bf16)

    pltpu.make_async_copy(mv, mv, in_sem.at[3]).wait()
    pltpu.make_async_copy(kvw, kvw, in_sem.at[4]).wait()
    for n in range(2):
        mb[y, k, q, n] = jnp.concatenate(
            [mv[n, 0, 0:8, :], mv[n, 1, 0:8, :], mv[n, 0, 8:16, :], mv[n, 1, 8:16, :]], axis=1
        )
    wb[k, q] = kvw[...].astype(bf16)

    with jax.named_scope("w_barrier"):
        pl.semaphore_wait(barrier, len(sources))

    tp = stage("tp", [(msend.at[yp(d)], yrecv.at[d - 1], at_y(d)) for d in (2, 1, 3)], yrecv)

    def signal(n, to):
        pl.semaphore_signal(ahead.at[n], inc=1, device_id=to, device_id_type=pl.DeviceIdType.MESH)

    signal(0, at_z(2))
    signal(0, at_z(14))

    load_x.wait()
    for n in range(4):
        wtt[pl.ds(n * 128, 128), :] = wt[:, n * 128 : (n + 1) * 128].T

    def start_far(d):
        remote(mb.at[y, k, q], mb.at[y, k, q], send_sem["mf"], recv_sem["mf"], at_z(d)).start()
        remote(wb.at[k, q], wb.at[k, q], send_sem["wf"], recv_sem["wf"], at_z(d)).start()

    with jax.named_scope("w_f1"):
        pl.semaphore_wait(ahead.at[0], 2)
    signal(1, at_z(4))
    signal(1, at_z(12))
    start_far(4)
    start_far(12)
    with jax.named_scope("w_f2"):
        pl.semaphore_wait(ahead.at[1], 2)
    start_far(8)
    three = mb.at[0, 0, pl.ds(0, 3)]
    m_far = remote(three, three, send_sem["mf"], recv_sem["mf"], partner)
    three = wb.at[0, pl.ds(0, 3)]
    w_far = remote(three, three, send_sem["wf"], recv_sem["wf"], partner)

    with jax.named_scope("w_tp"):
        tp.wait_recv()
    own = msend[y].astype(f32)
    for n in range(3):
        own = own + yrecv[n].astype(f32)
    swapped = pltpu.roll(own, 64, 1)
    low = lax.broadcasted_iota(jnp.int32, (HALF, 128), 1) < 64
    both = jnp.concatenate([jnp.where(low, own, swapped), jnp.where(low, swapped, own)], axis=0)
    upper = both.astype(bf16).astype(f32)
    first_half = lax.broadcasted_iota(jnp.int32, (TOK, 128), 1) < 64
    stream = jnp.where(first_half, upper, both - upper).astype(bf16).T
    low_tile = lax.broadcasted_iota(jnp.int32, (32, 8, 128), 2) < 64

    order = (14, 1, 15, 0)
    quarters = [lax.rem(zp(d), 4) for d in order]

    def product_of(n):
        cols = pl.ds(pl.multiple_of(quarters[n] * 512, 512), 512)
        wide = jnp.dot(stream, x_vm[:, cols], preferred_element_type=f32)
        part = wide[0:64] + wide[64:128]
        part = jnp.concatenate([part, part], axis=0).T.reshape(32, 2, 8, 128)
        packed = jnp.where(low_tile, part[:, 0], part[:, 1]).reshape(4, 8, 8, 128)
        for t in range(8):
            asend[n, t // 2, t % 2] = packed[:, t].reshape(32, 128).astype(bf16)
        copy = remote(asend.at[n, :, other], crecv.at[n], c_s.at[n], c_r.at[n], partner)
        copy.start()
        return copy

    to_core, to_x = [], []

    def core_to_x(n):
        with jax.named_scope(f"w_core{n}"):
            to_core[n].wait_recv()
        for t in range(NX):
            xsend[n, t] = (asend[n, t, c].astype(f32) + crecv[n, t].astype(f32)).astype(bf16)
        for d in (2, 1, 3):
            remote(xsend.at[n, xp(d)], xrecv.at[n, d - 1], x_s.at[n], x_r.at[n], at_x(d)).start()
        to_x.append(remote(xrecv.at[n], xrecv.at[n], x_s.at[n], x_r.at[n], partner))

    for n in range(3):
        to_core.append(product_of(n))
    core_to_x(0)
    to_core.append(product_of(3))
    for n in range(1, 4):
        core_to_x(n)

    for n in range(4):
        with jax.named_scope(f"w_x{n}"):
            to_x[n].wait_recv()
        total = xsend[n, x].astype(f32)
        for i in range(3):
            total = total + xrecv[n, i].astype(f32)
        if n < 3:
            tsend[n] = total.astype(bf16)
            remote(tsend.at[n], arecv.at[n], send_sem["a"], recv_sem["a"], at_z(order[n])).start()
    near = remote(arecv, arecv, send_sem["a"], recv_sem["a"], partner)

    with jax.named_scope("w_a"):
        near.wait_recv()
    for n in range(3):
        total = total + arecv[n].astype(f32)
    brecv[k] = total.astype(bf16)
    far = stage("b", [(brecv.at[k], brecv.at[k], at_z(d)) for d in (8, 4, 12)], brecv.at[pl.ds(0, 3)])
    with jax.named_scope("w_bg_far"):
        m_far.wait_recv()
    m_near = stage("mn", [(mb.at[y, :, q], mb.at[y, :, q], at_z(d)) for d in (14, 1, 15)], mb.at[0, pl.ds(0, 3)])

    with jax.named_scope("w_bg_near"):
        m_near.wait_recv()
    m_tp = stage("my", [(mb.at[y], mb.at[y], at_y(d)) for d in (2, 1, 3)], mb.at[pl.ds(0, 3)])

    with jax.named_scope("w_bg_wf"):
        w_far.wait_recv()
    w_near = stage("wn", [(wb.at[:, q], wb.at[:, q], at_z(d)) for d in (14, 1, 15)], wb.at[pl.ds(0, 3)])
    with jax.named_scope("w_b"):
        far.wait_recv()
    total = brecv[0].astype(f32)
    for n in range(1, 4):
        total = total + brecv[n].astype(f32)
    rounded = total.astype(bf16)
    gy[y, q] = rounded
    rounded = rounded.astype(f32)

    def spot(residue, yy, which):
        return (residue * NY + yy) * (NX * NC) + which

    mine = sb.at[spot(q, y, xc)]
    mine[...] = jnp.sum(rounded * rounded, axis=0, keepdims=True)
    around = sorted(
        ((dz, dx, dc, dy) for dz in (14, 15, 1, 0) for dx in range(NX) for dc in range(NC) for dy in range(NY)),
        key=lambda d: -(min(d[0], NZ - d[0]) + min(d[1], NX - d[1]) + min(d[3], NY - d[3]) + d[2] * 0.5),
    )[:-1]

    def start_squares(some):
        for dz, dx, dc, dy in some:
            to = (zp(dz), xp(dx), c if dc == 0 else other, yp(dy))
            remote(mine, mine, send_sem["sq"], recv_sem["sq"], to).start()

    start_squares(around)
    part = gy.at[y, q]
    for dz in (14, 1, 15, 0):
        for dy in (2, 1, 3):
            remote(part, part, send_sem["h"], recv_sem["h"], (zp(dz), x, c, yp(dy))).start()
    spread = stage("g", [(part, part, at_z(d)) for d in (14, 1, 15)], arecv)
    across = remote(gy.at[pl.ds(0, 3)], gy.at[pl.ds(0, 3)], send_sem["h"], recv_sem["h"], partner)
    every = sb.at[pl.ds(0, len(around))]
    squares = remote(every, every, send_sem["sq"], recv_sem["sq"], partner)

    with jax.named_scope("w_bg_y"):
        m_tp.wait_recv()
    with jax.named_scope("w_c"):
        spread.wait_recv()
    with jax.named_scope("w_y"):
        across.wait_recv()
    with jax.named_scope("w_s"):
        squares.wait_recv()

    total_sq = jnp.sum(jnp.sum(sb[...], axis=0), axis=1, keepdims=True)
    clip_limit = clip_target * jnp.sqrt(jnp.float32(2 * D * RANK))
    clip_factor = jnp.minimum(1.0, clip_limit / jnp.sqrt(total_sq + norm_eps))

    left, right = at_x(3), at_x(1)
    xc_left, xc_right, xc_across = xp(3) * 2 + c, xp(1) * 2 + c, xp(2) * 2 + c
    piece = wb.at[0]

    def send_piece(part, which, send, recv, to):
        for ref in (ko_ref, vo_ref):
            at = ref.at[pl.ds(part * 4, 4), which]
            remote(at, at, send, recv, to).start()

    go_right, go_left = [], []

    def to_right(part, which):
        n = len(go_right)
        send_piece(part, which, o_s.at[n], o_r.at[n], right)
        go_right.append(remote(piece, piece, o_s.at[n], o_r.at[n], right))

    def to_left(part, which):
        n = 6 + len(go_left)
        send_piece(part, which, o_s.at[n], o_r.at[n], left)
        go_left.append(remote(piece, piece, o_s.at[n], o_r.at[n], left))

    def to_partner(part, which):
        send_piece(part, which, o_s.at[12], o_r.at[12], partner)

    for batch in ((0, 3), (1, 2)):
        rows = []
        for part in batch:
            pieces = []
            for t in range(NY):
                scaled = clip_factor * gy[t, part].astype(f32)
                first_new = beta_first * mb[t, part, :, 0].reshape(32, 128) + (1.0 - beta_first) * scaled
                second_new = beta_second * mb[t, part, :, 1].reshape(32, 128) + (1.0 - beta_second) * scaled * scaled
                firsts[t, pl.ds(part * 4, 4)] = first_new.reshape(4, 8, 128)
                seconds[t, pl.ds(part * 4, 4)] = second_new.reshape(4, 8, 128)
                pieces.append(first_new / (jnp.sqrt(second_new) + small_eps))
            rows.append(jnp.concatenate(pieces, axis=1))
        direction = jnp.concatenate(rows, axis=0)
        upper = direction.astype(bf16)
        lower = (direction - upper.astype(f32)).astype(bf16)
        product = jnp.dot(jnp.concatenate([upper, lower], axis=0), wtt[...], preferred_element_type=f32)
        product = product[0:64] + product[64:128]
        if batch[0] == 0:
            with jax.named_scope("w_bg_wn"):
                w_near.wait_recv()
        for n, part in enumerate(batch):
            change = product[n * 32 : n * 32 + 32]
            upd[pl.ds(part * 4, 4)] = change.reshape(4, 8, 2 * NW)
            moved = jnp.stack(
                [change[:, 0:NW].reshape(4, 8, NW), change[:, NW : 2 * NW].reshape(4, 8, NW)], axis=1
            ).reshape(4, 16, NW)
            new = (wb[part].astype(f32) - step_rate * moved).astype(bf16)
            ko_ref[pl.ds(part * 4, 4), xc] = new[:, :, 0:NK]
            vo_ref[pl.ds(part * 4, 4), xc] = new[:, :, NK:NW]
        if batch[0] == 0:
            to_right(0, xc)
            to_left(3, xc)
        else:
            to_right(1, xc)
            to_left(2, xc)
            to_right(2, xc)
            to_left(1, xc)
            to_right(3, xc)
            to_left(0, xc)
        for part in batch:
            to_partner(part, xc)

    for out, packed_all in ((first_ref, firsts), (second_ref, seconds)):
        packed = packed_all[y, z]
        out[0, 0:8, :] = packed[:, 0:32]
        out[1, 0:8, :] = packed[:, 32:64]
        out[0, 8:16, :] = packed[:, 64:96]
        out[1, 8:16, :] = packed[:, 96:128]
    own_upd = upd[z]
    for half in range(2):
        rows = slice(half * 8, half * 8 + 8)
        at = half * NW
        nk_ref[rows, :] = kvw[rows, 0:NK] - step_rate * own_upd[:, at : at + NK]
        nv_ref[rows, :] = kvw[rows, NK:NW] - step_rate * own_upd[:, at + NK : at + NW]

    finish.extend([near, across, squares, m_far, w_far])
    for copy in to_core + to_x + finish:
        copy.wait_send()

    for n in range(6):
        with jax.named_scope(f"w_r{n}"):
            go_right[n].wait_recv()
        if n < 2:
            to_right(n, xc_left)
        to_partner(n % 4, xc_left if n < 4 else xc_across)
        with jax.named_scope(f"w_l{n}"):
            go_left[n].wait_recv()
        if n < 2:
            to_left(3 - n, xc_right)
        to_partner(3 - n % 4, xc_right if n < 4 else xc_across)
    with jax.named_scope("w_osend"):
        for copy in go_right + go_left:
            copy.wait_send()
    with jax.named_scope("w_oc"):
        both_ways = vo_ref.at[pl.ds(0, 12)]
        last = remote(both_ways, both_ways, o_s.at[12], o_r.at[12], partner)
        last.wait_recv()
        last.wait_send()


def store(*refs):
    sems = refs[-1]
    count = (len(refs) - 1) // 2
    copies = [pltpu.make_async_copy(refs[n], refs[count + n], sems.at[n]) for n in range(count)]
    for copy in reversed(copies):
        copy.start()
    for copy in copies:
        copy.wait()


def local(*args):
    vmem = pl.BlockSpec(memory_space=pltpu.VMEM)
    hbm = pl.BlockSpec(memory_space=pltpu.HBM)
    dma = pltpu.SemaphoreType.DMA
    shape = jax.ShapeDtypeStruct
    outs = pl.pallas_call(
        kernel,
        out_shape=(
            shape((2, 16, 32), f32),
            shape((2, 16, 32), f32),
            shape((16, NK), f32),
            shape((16, NV), f32),
            shape((NZ, NX * NC, 16, NK), bf16),
            shape((NZ, NX * NC, 16, NV), bf16),
        ),
        in_specs=[hbm] * 9,
        out_specs=[vmem] * 6,
        scratch_shapes=[
            pltpu.VMEM((TOK, D), bf16),
            pltpu.VMEM((TOK, NW), bf16),
            pltpu.VMEM((NW, RANK), bf16),
            pltpu.VMEM((16, NW), f32),
            pltpu.VMEM((2, 2, 16, 32), f32),
            pltpu.VMEM((2 * NW, 4 * 128), bf16),
            pltpu.VMEM((4 * 128, 2 * NW), bf16),
            pltpu.VMEM((NY, HALF, 128), bf16),
            pltpu.VMEM((NY - 1, HALF, 128), bf16),
            pltpu.VMEM((4, NX, NC, 32, 128), bf16),
            pltpu.VMEM((4, NX, 32, 128), bf16),
            pltpu.VMEM((4, NX, 32, 128), bf16),
            pltpu.VMEM((4, NX - 1, 32, 128), bf16),
            pltpu.VMEM((3, 32, 128), bf16),
            pltpu.VMEM((3, 32, 128), bf16),
            pltpu.VMEM((4, 32, 128), bf16),
            pltpu.VMEM((NY, 4, 32, 128), bf16),
            pltpu.VMEM((NY, 4, 4, 2, 8, 128), f32),
            pltpu.VMEM((4, 4, 16, NW), bf16),
            pltpu.VMEM((4 * NY * NX * NC, 1, 128), f32),
            pltpu.VMEM((NY, 16, 8, 128), f32),
            pltpu.VMEM((NY, 16, 8, 128), f32),
            pltpu.VMEM((16, 8, 2 * NW), f32),
            dma((5,)), pltpu.SemaphoreType.REGULAR((2,)), dma((4,)), dma((4,)), dma((4,)), dma((4,)), dma((13,)), dma((13,)), dma((11,)), dma((11,)),
        ],
        compiler_params=pltpu.CompilerParams(
            collective_id=0, has_side_effects=True, vmem_limit_bytes=40 * 1024 * 1024
        ),
        name="step",
    )(*[pltpu.with_memory_space_constraint(a, pltpu.HBM) for a in args])
    results = (*outs[:4], outs[4].reshape(D, NK), outs[5].reshape(D, NV))
    return pl.pallas_call(
        store,
        out_shape=tuple(shape(r.shape, r.dtype) for r in results),
        in_specs=[pl.BlockSpec(memory_space=pl.ANY)] * 6,
        out_specs=[hbm] * 6,
        scratch_shapes=[dma((6,))],
        compiler_params=pltpu.CompilerParams(vmem_limit_bytes=1024 * 1024),
        name="store",
    )(*results)


def solution(mesh):
    torus = Mesh(mesh.devices.reshape(NZ, NX, NC, NY), ("z", "x", "c", "y"))
    return jax.shard_map(
        local,
        mesh=torus,
        in_specs=(
            P(FS, None), P(FS, "y"), P(FS, "y"), P("y", None), P("y", None), P(FS, "y"), P(FS, "y"),
            P(None, FS, "y"), P(None, FS, "y"),
        ),
        out_specs=(P(None, FS, "y"), P(None, FS, "y"), P(FS, "y"), P(FS, "y"), P(None, "y"), P(None, "y")),
        check_vma=False,
    )
```
